512 devices in a mesh: ra: 16 (over z), cb: 4 (over y), dp: 8 (over x, core).
Axes of the slice: x: 4, y: 4, z: 16, core: 2. Of those that a mesh axis runs over, the one named last changes fastest.
Arguments:
- tokens: bfloat16 [8, 512, 4096], P('dp', None, 'ra'), may hold values from -80 to 80
- pre_gain: float32 [4096], P('ra'), may hold values from 0.1 to 1.9
- w_gate: bfloat16 [4096, 11264], P('ra', 'cb'), may hold values from -0.09375 to 0.09375
- w_up: bfloat16 [4096, 11264], P('ra', 'cb'), may hold values from -0.09375 to 0.09375
- conv_gate: float32 [3, 11264], P(None, 'cb'), may hold values from -3.5 to 3.5
- conv_up: float32 [3, 11264], P(None, 'cb'), may hold values from -3.5 to 3.5
- w_down: bfloat16 [11264, 4096], P('cb', 'ra'), may hold values from -2 to 2
- post_gain: float32 [4096], P('ra'), may hold values from 0.1 to 1.9
Outputs:
- mixed: bfloat16 [8, 512, 4096], P('dp', None, 'ra')
The draws below stay inside these ranges and needn't reach their ends.
All inputs are finite; a program needn't handle non-finite values.
Results may differ from the reference program's by a relative error of at most 0.0064.
Values may be sent and summed in bfloat16 or wider, within the bound.
A program may use at most 64 MiB of HBM per device.

```python
import math
import jax
import jax.numpy as jnp
from jax import lax

D = 4096
FF = 11264
TOK_DEV = 512
SEQS = 8


def column_scales(key, width):
    column = jnp.arange(width, dtype=jnp.float32) / (width - 1)
    return 10.0 ** column * jax.random.uniform(key, (width,), jnp.float32, 0.7, 1.4) / 4.0


def draw_tokens(key, part):
    first, second, third = jax.random.split(jax.random.fold_in(key, 11), 3)
    col_scale = column_scales(second, D)
    base = jnp.clip(jax.random.normal(first, (SEQS, TOK_DEV, D), jnp.float32), -6.0, 6.0)
    row_scale = jnp.exp(jax.random.uniform(third, (SEQS, TOK_DEV, 1), jnp.float32, 0.0, math.log(10.0)))
    return (base * row_scale * col_scale / 3.0).astype(jnp.bfloat16)


def draw_w_down(key, part):
    first, second = jax.random.split(jax.random.fold_in(key, 23), 2)
    col_scale = column_scales(second, D)
    base = jnp.clip(jax.random.normal(first, (FF, D), jnp.float32), -6.0, 6.0)
    return (base * col_scale / math.sqrt(FF)).astype(jnp.bfloat16)


def levels(key, extent, cuts, least, top_value):
    level = 1.0
    for axis_at, shards_of in cuts:
        draws = jax.random.uniform(jax.random.fold_in(jax.random.fold_in(key, 6), axis_at), (shards_of,), jnp.float32, least / len(cuts), top_value / len(cuts))
        level = level * jnp.repeat(jnp.exp(draws), extent[axis_at] // shards_of).reshape((-1,) + (1,) * (len(extent) - 1 - axis_at))
    return level


def normal_values(rng, dims, spread, reach, pieces=(), kind=jnp.bfloat16):
    gain = levels(rng, dims, pieces, -0.22, 0.18) if pieces else 1.0
    entries = jax.random.normal(rng, dims, jnp.float32) * spread * gain
    return jnp.minimum(jnp.maximum(entries, -reach), reach).astype(kind)


def setup_inputs(seed: int = 0) -> dict:
    key_list = jax.random.split(jax.random.key(seed), 9)
    return {
        "tokens": draw_tokens(jax.random.fold_in(key_list[8], 71), 0),
        "pre_gain": jnp.clip(1.0 + 0.18 * jax.random.normal(key_list[1], (D,), jnp.float32), 0.1, 1.9),
        "w_gate": normal_values(key_list[2], (D, FF), D ** -0.5, 0.09375, ((0, 16), (1, 4))),
        "w_up": normal_values(key_list[3], (D, FF), D ** -0.5, 0.09375, ((0, 16), (1, 4))),
        "conv_gate": normal_values(key_list[4], (3, FF), 3 ** -0.5, 3.5, ((1, 4),), jnp.float32),
        "conv_up": normal_values(key_list[5], (3, FF), 3 ** -0.5, 3.5, ((1, 4),), jnp.float32),
        "w_down": draw_w_down(jax.random.fold_in(key_list[8], 71), 0),
        "post_gain": jnp.clip(1.0 + 0.18 * jax.random.normal(key_list[7], (D,), jnp.float32), 0.1, 1.9),
    }


epsilon = 1e-06
residual_scale = 0.125

def shifted_sum(field, tap_weights):
    padded = jnp.pad(field, ((0, 0), (1, 1), (0, 0)))
    return padded[:, :-2] * tap_weights[0] + padded[:, 1:-1] * tap_weights[1] + padded[:, 2:] * tap_weights[2]

def reference(tokens, pre_gain, w_gate, w_up, conv_gate, conv_up, w_down, post_gain):
    seq_count, positions, features = tokens.shape
    values = tokens.astype(jnp.float32)
    pre_scale = lax.rsqrt(lax.optimization_barrier(jnp.mean(values * values, axis=-1, keepdims=True)) + epsilon)
    weighted = (values * pre_gain).astype(jnp.bfloat16).reshape(seq_count * positions, features)
    gate_lin = jnp.dot(weighted, w_gate, preferred_element_type=jnp.float32).reshape(seq_count, positions, -1) * pre_scale
    up_lin = jnp.dot(weighted, w_up, preferred_element_type=jnp.float32).reshape(seq_count, positions, -1) * pre_scale
    gate_conv = shifted_sum(gate_lin, conv_gate)
    up_conv = shifted_sum(up_lin, conv_up)
    hidden = (jax.nn.gelu(gate_conv, approximate=True) * up_conv).astype(jnp.bfloat16)
    branch = jnp.dot(hidden.reshape(seq_count * positions, -1), w_down, preferred_element_type=jnp.float32)
    branch = branch.reshape(seq_count, positions, features)
    post_scale = lax.rsqrt(lax.optimization_barrier(jnp.mean(branch * branch, axis=-1, keepdims=True)) + epsilon)
    mixed = residual_scale * values + branch * post_scale * post_gain
    return mixed.astype(jnp.bfloat16)
```

```python
import functools
import jax
import jax.numpy as jnp
from jax import lax
from jax.experimental import pallas as pl
from jax.experimental.pallas import tpu as pltpu
from jax.sharding import PartitionSpec as P

EPS = 1e-06
RESIDUAL = 0.125
MESH = pl.DeviceIdType.MESH
BF16 = jnp.bfloat16
F32 = jnp.float32


def _kernel(
    dim_full,
    nz,
    xw_ref, sq_ref, ws_ref, taps_ref, wd_ref, tok_ref, gain_ref,
    out_ref,
    xfull, wfull, hfull, acc, part, psend, precv, sq_all, psq_own, psq_all, mshare,
    xz_s, xz_r, y1_s, y1_r, y2_s, y2_r, wz_s, wz_r, wx_s, wx_r, wo_s, wo_r, wp_s, wp_r,
    sq_s, sq_r, hz_s, hz_r, ps_s, ps_r, pq_s, pq_r, mo_s, mo_r,
):
    half = nz // 2
    z = lax.axis_index("ra")
    y = lax.axis_index("cb")
    dp = lax.axis_index("dp")
    tokens, kb = xw_ref.shape
    quarter = tokens // 4
    qhalf = quarter // 2
    units = hfull.shape[2]
    hcols = hfull.shape[3]

    def zmod(v):
        return lax.rem(v + 2 * nz, nz)

    z_right, z_left = zmod(z + 1), zmod(z - 1)
    y_right, y_left, y_far = lax.rem(y + 1, 4), lax.rem(y + 3, 4), lax.rem(y + 2, 4)
    x_right, x_left = lax.rem(dp + 2, 8), lax.rem(dp + 6, 8)
    x_far = lax.rem(dp + 4, 8)
    partner = dp + 1 - 2 * lax.rem(dp, 2)

    def other(v):
        return v + 1 - 2 * lax.rem(v, 2)

    def rcopy(src, dst, ssem, rsem, dev):
        return pltpu.make_async_remote_copy(
            src_ref=src, dst_ref=dst, send_sem=ssem, recv_sem=rsem,
            device_id=dev, device_id_type=MESH,
        )

    bar = pltpu.get_barrier_semaphore()

    @pl.loop(1, nz)
    def _(d):
        pl.semaphore_signal(bar, inc=1, device_id={"ra": zmod(z + d)}, device_id_type=MESH)

    for t in (y_right, y_left, y_far):
        pl.semaphore_signal(bar, inc=1, device_id={"cb": t}, device_id_type=MESH)
    for t in (x_right, x_left, partner):
        pl.semaphore_signal(bar, inc=1, device_id={"dp": t}, device_id_type=MESH)
    pl.semaphore_wait(bar, nz - 1 + 6)

    def q_rows(q):
        return pl.ds(pl.multiple_of(q * quarter, quarter), quarter)

    def qh_rows(q, i):
        return pl.ds(pl.multiple_of(q * quarter + i * qhalf, qhalf), qhalf)

    def xz_copy(b, right, src=None):
        dst = xfull.at[b, q_rows(y)]
        return rcopy(dst if src is None else src, dst, xz_s.at[1 - right, b], xz_r.at[b],
                     {"ra": z_right if right else z_left})

    def y1_copy(b, right, q):
        ref = xfull.at[b, q_rows(q)]
        return rcopy(ref, ref, y1_s.at[1 - right, b], y1_r.at[1 - right, b],
                     {"cb": y_right if right else y_left})

    def y2_copy(b, right, q):
        ref = xfull.at[b, qh_rows(q, 1 - right)]
        return rcopy(ref, ref, y2_s.at[1 - right, b], y2_r.at[1 - right, b],
                     {"cb": y_right if right else y_left})

    def wz_copy(dest, source):
        return rcopy(ws_ref.at[dest], wfull.at[source, dp], wz_s.at[dest], wz_r.at[source],
                     {"ra": dest})

    def wx_copy(b, right, share, src=None):
        ref = wfull.at[b, share]
        return rcopy(ref if src is None else src, ref, wx_s.at[1 - right, b], wx_r.at[1 - right, b],
                     {"dp": x_right if right else x_left})

    def wo_copy(b, right, share):
        ref = wfull.at[b, share]
        return rcopy(ref, ref, wo_s.at[b], wo_r.at[b], {"dp": x_right if right else x_left})

    def wp_copy(b, k, share, src=None):
        ref = wfull.at[b, share]
        return rcopy(ref if src is None else src, ref, wp_s.at[k, b], wp_r.at[k, b], {"dp": partner})

    def sq_copy(dest, source):
        return rcopy(sq_ref, sq_all.at[source], sq_s.at[dest], sq_r.at[source], {"ra": dest})

    def w_issue(d):
        wz_copy(zmod(z + d), z).start()

        @pl.when(d < half)
        def _():
            wz_copy(zmod(z - d), z).start()

    def both(d, fn):
        fn(zmod(z - d))

        @pl.when((d > 0) & (d < half))
        def _():
            fn(zmod(z + d))

    def w_arrive(b):
        wz_copy(b, b).wait_recv()
        wp_copy(b, 0, dp).start()
        wx_copy(b, 1, dp).start()
        wx_copy(b, 0, dp).start()

    def w_side(b):
        wx_copy(b, 1, x_left).wait_recv()
        wx_copy(b, 0, x_right).wait_recv()
        wp_copy(b, 1, x_left).start()
        wp_copy(b, 2, x_right).start()

        @pl.when(lax.rem(b, 2) == 0)
        def _():
            wo_copy(b, 1, x_left).start()

        @pl.when(lax.rem(b, 2) == 1)
        def _():
            wo_copy(b, 0, x_right).start()

    def w_far(b):
        wo_copy(b, 1, x_far).wait_recv()
        wp_copy(b, 3, x_far).start()

    def w_last(b):
        wp_copy(b, 0, partner).wait_recv()
        wp_copy(b, 1, other(x_left)).wait_recv()
        wp_copy(b, 2, other(x_right)).wait_recv()
        wp_copy(b, 3, other(x_far)).wait_recv()

    def x_first(b):
        y1_copy(b, 1, y).start()
        y1_copy(b, 0, y).start()

    def x_second(b):
        y1_copy(b, 1, y_left).wait_recv()
        y2_copy(b, 1, y_left).start()
        y1_copy(b, 0, y_right).wait_recv()
        y2_copy(b, 0, y_right).start()

    def x_third(b):
        y2_copy(b, 1, y_far).wait_recv()
        y2_copy(b, 0, y_far).wait_recv()

    xz_copy(z, 1, xw_ref.at[q_rows(y)]).start()
    xz_copy(z, 0, xw_ref.at[q_rows(y)]).start()
    w_issue(1)
    w_issue(2)
    wp_copy(z, 0, dp, ws_ref.at[z]).start()
    wx_copy(z, 1, dp, ws_ref.at[z]).start()
    wx_copy(z, 0, dp, ws_ref.at[z]).start()

    @pl.loop(1, nz)
    def _(d):
        sq_copy(zmod(z + d), z).start()

    wfull[z, dp] = ws_ref[z]
    sq_all[z] = sq_ref[...]
    xfull[z] = xw_ref[...]

    groups = half // 2

    def group(g, fn):
        both(2 * g - 1, fn)
        both(2 * g, fn)

    @pl.loop(1, half + 3)
    def _(s):
        @pl.when(s <= half)
        def _():
            br = zmod(z - s)
            xz_copy(br, 1).wait_recv()

            @pl.when(s < half)
            def _():
                xz_copy(br, 1).start()

            x_first(br)

            @pl.when(s < half)
            def _():
                bl = zmod(z + s)
                xz_copy(bl, 0).wait_recv()

                @pl.when(s < half - 1)
                def _():
                    xz_copy(bl, 0).start()

                x_first(bl)

        @pl.when(s < groups)
        def _():
            w_issue(2 * s + 1)
            w_issue(2 * s + 2)

        @pl.when((s >= 2) & (s <= half + 1))
        def _():
            both(s - 1, x_second)

        @pl.when(s >= 3)
        def _():
            both(s - 2, x_third)

        @pl.when(s == 2)
        def _():
            w_side(z)

        @pl.when(s == 3)
        def _():
            w_far(z)

        @pl.when((s >= 2) & (s < groups + 2))
        def _():
            group(s - 1, w_arrive)

        @pl.when((s >= 3) & (s < groups + 3))
        def _():
            group(s - 2, w_side)

        @pl.when((s >= 4) & (s < groups + 4))
        def _():
            group(s - 3, w_far)

    @pl.loop(0, half + 1)
    def _(d):
        both(d, w_last)

    acc[...] = jnp.zeros_like(acc)

    @pl.loop(0, nz)
    def _(b):
        w = wfull[b].reshape(kb, acc.shape[1])
        acc[...] += jnp.dot(xfull[b], w, preferred_element_type=F32)

    @pl.loop(1, nz)
    def _(d):
        src = zmod(z + d)
        sq_copy(src, src).wait_recv()

    scale = lax.rsqrt(jnp.sum(sq_all[...], axis=0) / dim_full + EPS)
    lin = jnp.transpose(acc[...], (1, 0))

    def conv(field, base):
        lane = lax.broadcasted_iota(jnp.int32, field.shape, 1)
        before = jnp.where(lane == 0, 0.0, pltpu.roll(field, 1, 1))
        after = jnp.where(lane == tokens - 1, 0.0, pltpu.roll(field, tokens - 1, 1))
        return (
            taps_ref[:, base : base + 1] * before
            + taps_ref[:, base + 1 : base + 2] * field
            + taps_ref[:, base + 2 : base + 3] * after
        )

    gate = conv(lin[:units] * scale, 0)
    up = conv(lin[units : 2 * units] * scale, 3)
    hidden = (jax.nn.gelu(gate, approximate=True) * up).astype(BF16)
    subs = tokens // hcols
    for c in range(subs):
        hfull[z, c] = hidden[:, c * hcols : (c + 1) * hcols]

    def hz_copy(b, c, right):
        ref = hfull.at[b, c]
        return rcopy(ref, ref, hz_s.at[1 - right, b, c], hz_r.at[b, c],
                     {"ra": z_right if right else z_left})

    for c in range(subs):
        hz_copy(z, c, 1).start()
        hz_copy(z, c, 0).start()

    def down(b, c, first=False):
        w = wd_ref[pl.ds(pl.multiple_of(b * units, units), units), :]
        value = lax.dot_general(w, hfull[b, c], (((0,), (0,)), ((), ())), preferred_element_type=F32)
        cols = pl.ds(c * hcols, hcols)
        if first:
            part[:, cols] = value
        else:
            part[:, cols] += value

    for c in range(subs):
        down(z, c, True)

    @pl.loop(1, half)
    def _(s):
        br, bl = zmod(z - s), zmod(z + s)
        for c in range(subs):
            hz_copy(br, c, 1).wait_recv()
            if c < subs // 2:
                hz_copy(br, c, 1).start()
            else:
                @pl.when(s < half - 1)
                def _():
                    hz_copy(br, c, 1).start()
            hz_copy(bl, c, 0).wait_recv()
            if c >= subs // 2:
                hz_copy(bl, c, 0).start()
            else:
                @pl.when(s < half - 1)
                def _():
                    hz_copy(bl, c, 0).start()
        for c in range(subs):
            down(br, c)
            down(bl, c)

    far = zmod(z + half)
    for c in range(subs):
        hz_copy(far, c, 1 if c < subs // 2 else 0).wait_recv()
        down(far, c)

    def ps_copy(k, dest):
        return rcopy(psend.at[k], precv.at[k], ps_s.at[k], ps_r.at[k], {"cb": dest})

    def quarter_cols(q):
        return pl.ds(pl.multiple_of(q * quarter, quarter), quarter)

    for k, dest in enumerate((y_far, y_right, y_left)):
        psend[k] = part[:, quarter_cols(dest)].astype(BF16)
        ps_copy(k, dest).start()
    share = part[:, quarter_cols(y)]
    for k, dest in enumerate((y_far, y_right, y_left)):
        ps_copy(k, dest).wait_recv()
        share = share + precv[k].astype(F32)

    def pq_copy(dest, source):
        return rcopy(psq_own, psq_all.at[source], pq_s.at[dest], pq_r.at[source], {"ra": dest})

    own_sq = jnp.sum(share * share, axis=0, keepdims=True)
    psq_own[...] = own_sq
    psq_all[z] = own_sq

    @pl.loop(1, nz)
    def _(d):
        pq_copy(zmod(z + d), z).start()

    branch = jnp.transpose(share, (1, 0)) * gain_ref[...]
    base = RESIDUAL * tok_ref[q_rows(y), :].astype(F32)

    @pl.loop(1, nz)
    def _(d):
        src = zmod(z + d)
        pq_copy(src, src).wait_recv()

    post = lax.rsqrt(jnp.sum(psq_all[...], axis=0) / dim_full + EPS)
    post_col = jnp.transpose(jnp.broadcast_to(post, (quarter, quarter)), (1, 0))[:, :1]
    mixed = (base + branch * post_col).astype(BF16)
    mshare[...] = mixed
    out_ref[q_rows(y), :] = mixed

    def mo_copy(k, dest, q):
        return rcopy(mshare, out_ref.at[q_rows(q)], mo_s.at[k], mo_r.at[k], {"cb": dest})

    for k, dest in enumerate((y_far, y_right, y_left)):
        mo_copy(k, dest, y).start()
    for k, source in enumerate((y_far, y_left, y_right)):
        mo_copy(k, source, source).wait_recv()

    @pl.loop(0, half + 1)
    def _(s):
        @pl.when(s < half)
        def _():
            xz_copy(zmod(z - s), 1).wait_send()
            hz_copy(zmod(z - s), 0, 1).wait_send()

        @pl.when(s < half - 1)
        def _():
            xz_copy(zmod(z + s), 0).wait_send()

        for c in range(subs):
            first = c < subs // 2

            @pl.when(s < (half if first else half - 1))
            def _():
                if c > 0:
                    hz_copy(zmod(z - s), c, 1).wait_send()

            @pl.when(s < (half - 1 if first else half))
            def _():
                hz_copy(zmod(z + s), c, 0).wait_send()

    @pl.loop(0, nz)
    def _(b):
        @pl.when(b != z)
        def _():
            y1_copy(b, 1, y).wait_send()
            y1_copy(b, 0, y).wait_send()
            y2_copy(b, 1, y_left).wait_send()
            y2_copy(b, 0, y_right).wait_send()
            wz_copy(b, z).wait_send()
            sq_copy(b, z).wait_send()
            pq_copy(b, z).wait_send()

        wx_copy(b, 1, dp).wait_send()
        wx_copy(b, 0, dp).wait_send()
        wo_copy(b, 1, x_left).wait_send()
        for k in range(4):
            wp_copy(b, k, dp).wait_send()

    for k, dest in enumerate((y_far, y_right, y_left)):
        ps_copy(k, dest).wait_send()
        mo_copy(k, dest, y).wait_send()


def local(tokens, pre_gain, w_gate, w_up, conv_gate, conv_up, w_down, post_gain):
    nz = lax.axis_size("ra")
    _, positions, kb = tokens.shape
    ff = w_gate.shape[1]
    units = ff // nz
    lanes = -(-2 * units // 128) * 128
    rows = kb // 8
    quarter = positions // 4
    subs = 2
    dim_full = kb * nz
    tok = tokens[0]
    values = tok.astype(F32)
    sq = jnp.sum(values * values, axis=1)[None, :]
    weighted = (values * pre_gain).astype(BF16)
    row = lax.axis_index("dp") * rows

    def pieces(w):
        own = lax.dynamic_slice_in_dim(w, row, rows, 0)
        return own.reshape(rows, nz, units).transpose(1, 0, 2)

    ws = jnp.concatenate(
        [pieces(w_gate), pieces(w_up), jnp.zeros((nz, rows, lanes - 2 * units), BF16)], axis=2
    )
    start = lax.axis_index("ra") * units
    taps = jnp.concatenate(
        [
            lax.dynamic_slice_in_dim(conv_gate, start, units, 1),
            lax.dynamic_slice_in_dim(conv_up, start, units, 1),
        ],
        axis=0,
    ).T

    dma = pltpu.SemaphoreType.DMA
    vmem = pltpu.VMEM
    scratch = [
        vmem((nz, positions, kb), BF16),
        vmem((nz, 8, rows, lanes), BF16),
        vmem((nz, subs, units, positions // subs), BF16),
        vmem((positions, lanes), F32),
        vmem((kb, positions), F32),
        vmem((3, kb, quarter), BF16),
        vmem((3, kb, quarter), BF16),
        vmem((nz, 1, positions), F32),
        vmem((1, quarter), F32),
        vmem((nz, 1, quarter), F32),
        vmem((quarter, kb), BF16),
        dma((2, nz)), dma((nz,)),
        dma((2, nz)), dma((2, nz)), dma((2, nz)), dma((2, nz)),
        dma((nz,)), dma((nz,)), dma((2, nz)), dma((2, nz)), dma((nz,)), dma((nz,)),
        dma((4, nz)), dma((4, nz)),
        dma((nz,)), dma((nz,)), dma((2, nz, subs)), dma((nz, subs)),
        dma((3,)), dma((3,)), dma((nz,)), dma((nz,)), dma((3,)), dma((3,)),
    ]

    out = pl.pallas_call(
        functools.partial(_kernel, dim_full, nz),
        out_shape=jax.ShapeDtypeStruct((positions, kb), BF16),
        in_specs=[pl.BlockSpec(memory_space=pltpu.VMEM)] * 7,
        out_specs=pl.BlockSpec(memory_space=pltpu.VMEM),
        scratch_shapes=scratch,
        name="ffn",
        compiler_params=pltpu.CompilerParams(
            collective_id=0, has_side_effects=True, vmem_limit_bytes=48 * 1024 * 1024
        ),
    )(weighted, sq, ws, taps, w_down, tok, post_gain[None, :])
    return out[None]


def solution(mesh):
    in_specs = (
        P("dp", None, "ra"),
        P("ra"),
        P("ra", "cb"),
        P("ra", "cb"),
        P(None, "cb"),
        P(None, "cb"),
        P("cb", "ra"),
        P("ra"),
    )
    out_specs = P("dp", None, "ra")
    return jax.shard_map(local, mesh=mesh, in_specs=in_specs, out_specs=out_specs, check_vma=False)
```

```python
import functools
import jax
import jax.numpy as jnp
from jax import lax
from jax.experimental import pallas as pl
from jax.experimental.pallas import tpu as pltpu
from jax.sharding import PartitionSpec as P

EPS = 1e-06
RESIDUAL = 0.125
MESH = pl.DeviceIdType.MESH
BF16 = jnp.bfloat16
F32 = jnp.float32


def _kernel(
    dim_full,
    nz,
    tok_ref, pre_ref, wg_ref, wu_ref, cg_ref, cu_ref, wd_hbm, gain_ref,
    out_ref,
    xw_ref, sq_ref, ws_ref, wrows, wd_ref, taps_in, taps_ref,
    xfull, wfull, hfull, acc, part, psend, precv, sq_all, psq_own, psq_all,
    bshare, bfull, post_own, post_all, in_sem,
    xz_s, xz_r, y1_s, y1_r, y2_s, y2_r, wz_s, wz_r, wx_s, wx_r, wo_s, wo_r, wp_s, wp_r,
    sq_s, sq_r, hz_s, hz_r, ps_s, ps_r, pq_s, pq_r, mo_s, mo_r, po_s, po_r,
):
    half = nz // 2
    z = lax.axis_index("ra")
    y = lax.axis_index("cb")
    dp = lax.axis_index("dp")
    tokens, kb = xw_ref.shape
    quarter = tokens // 4
    qhalf = quarter // 2
    units = hfull.shape[1]
    rows = wrows.shape[1]
    lanes = acc.shape[1]

    def zmod(v):
        return lax.rem(v + 2 * nz, nz)

    z_right, z_left = zmod(z + 1), zmod(z - 1)
    y_right, y_left, y_far = lax.rem(y + 1, 4), lax.rem(y + 3, 4), lax.rem(y + 2, 4)
    x_right, x_left = lax.rem(dp + 2, 8), lax.rem(dp + 6, 8)
    x_far = lax.rem(dp + 4, 8)
    partner = dp + 1 - 2 * lax.rem(dp, 2)

    def other(v):
        return v + 1 - 2 * lax.rem(v, 2)

    def rcopy(src, dst, ssem, rsem, dev):
        return pltpu.make_async_remote_copy(
            src_ref=src, dst_ref=dst, send_sem=ssem, recv_sem=rsem,
            device_id=dev, device_id_type=MESH,
        )

    bar = pltpu.get_barrier_semaphore()

    @pl.loop(1, nz)
    def _(d):
        pl.semaphore_signal(bar, inc=1, device_id={"ra": zmod(z + d)}, device_id_type=MESH)

    for t in (y_right, y_left, y_far):
        pl.semaphore_signal(bar, inc=1, device_id={"cb": t}, device_id_type=MESH)
    for t in (x_right, x_left, partner):
        pl.semaphore_signal(bar, inc=1, device_id={"dp": t}, device_id_type=MESH)

    own = pl.ds(pl.multiple_of(dp * rows, rows), rows)
    loads = [
        pltpu.make_async_copy(wg_ref.at[own], wrows.at[0], in_sem.at[0]),
        pltpu.make_async_copy(wu_ref.at[own], wrows.at[1], in_sem.at[1]),
        pltpu.make_async_copy(wd_hbm, wd_ref, in_sem.at[2]),
    ]
    for load in loads:
        load.start()
    values = tok_ref[...].astype(F32)
    xw_ref[...] = (values * pre_ref[...]).astype(BF16)
    sq_ref[...] = jnp.sum(jnp.transpose(values * values, (1, 0)), axis=0, keepdims=True)
    loads[0].wait()
    loads[1].wait()
    tail = jnp.zeros((rows, lanes - 2 * units), BF16)
    for j in range(nz):
        cut = slice(j * units, (j + 1) * units)
        ws_ref[j] = jnp.concatenate([wrows[0, :, cut], wrows[1, :, cut], tail], axis=1)
    xfull[z] = xw_ref[...]
    wfull[z, dp] = ws_ref[z]
    sq_all[z] = sq_ref[...]
    pl.semaphore_wait(bar, nz - 1 + 6)

    def q_rows(q):
        return pl.ds(pl.multiple_of(q * quarter, quarter), quarter)

    def qh_rows(q, i):
        return pl.ds(pl.multiple_of(q * quarter + i * qhalf, qhalf), qhalf)

    def xz_copy(b, right, src=None):
        dst = xfull.at[b, q_rows(y)]
        return rcopy(dst if src is None else src, dst, xz_s.at[1 - right, b], xz_r.at[b],
                     {"ra": z_right if right else z_left})

    def y1_copy(b, right, q):
        ref = xfull.at[b, q_rows(q)]
        return rcopy(ref, ref, y1_s.at[1 - right, b], y1_r.at[1 - right, b],
                     {"cb": y_right if right else y_left})

    def y2_copy(b, right, q):
        ref = xfull.at[b, qh_rows(q, 1 - right)]
        return rcopy(ref, ref, y2_s.at[1 - right, b], y2_r.at[1 - right, b],
                     {"cb": y_right if right else y_left})

    def wz_copy(dest, source):
        return rcopy(ws_ref.at[dest], wfull.at[source, dp], wz_s.at[dest], wz_r.at[source],
                     {"ra": dest})

    def wx_copy(b, right, share, src=None):
        ref = wfull.at[b, share]
        return rcopy(ref if src is None else src, ref, wx_s.at[1 - right, b], wx_r.at[1 - right, b],
                     {"dp": x_right if right else x_left})

    def wo_copy(b, right, share):
        ref = wfull.at[b, share]
        return rcopy(ref, ref, wo_s.at[b], wo_r.at[b], {"dp": x_right if right else x_left})

    def wp_copy(b, k, share, src=None):
        ref = wfull.at[b, share]
        return rcopy(ref if src is None else src, ref, wp_s.at[k, b], wp_r.at[k, b], {"dp": partner})

    def sq_copy(dest, source):
        return rcopy(sq_ref, sq_all.at[source], sq_s.at[dest], sq_r.at[source], {"ra": dest})

    def w_issue(d):
        wz_copy(zmod(z + d), z).start()

        @pl.when(d < half)
        def _():
            wz_copy(zmod(z - d), z).start()

    def both(d, fn):
        fn(zmod(z - d))

        @pl.when((d > 0) & (d < half))
        def _():
            fn(zmod(z + d))

    def w_arrive(b):
        wz_copy(b, b).wait_recv()
        wp_copy(b, 0, dp).start()
        wx_copy(b, 1, dp).start()
        wx_copy(b, 0, dp).start()

    def w_side(b):
        wx_copy(b, 1, x_left).wait_recv()
        wx_copy(b, 0, x_right).wait_recv()
        wp_copy(b, 1, x_left).start()
        wp_copy(b, 2, x_right).start()

        @pl.when(lax.rem(b, 2) == 0)
        def _():
            wo_copy(b, 1, x_left).start()

        @pl.when(lax.rem(b, 2) == 1)
        def _():
            wo_copy(b, 0, x_right).start()

    def w_far(b):
        wo_copy(b, 1, x_far).wait_recv()
        wp_copy(b, 3, x_far).start()

    def w_last(b):
        wp_copy(b, 0, partner).wait_recv()
        wp_copy(b, 1, other(x_left)).wait_recv()
        wp_copy(b, 2, other(x_right)).wait_recv()
        wp_copy(b, 3, other(x_far)).wait_recv()

    def x_first(b):
        y1_copy(b, 1, y).start()
        y1_copy(b, 0, y).start()

    def x_second(b):
        y1_copy(b, 1, y_left).wait_recv()
        y2_copy(b, 1, y_left).start()
        y1_copy(b, 0, y_right).wait_recv()
        y2_copy(b, 0, y_right).start()

    def x_third(b):
        y2_copy(b, 1, y_far).wait_recv()
        y2_copy(b, 0, y_far).wait_recv()

    xz_copy(z, 1, xw_ref.at[q_rows(y)]).start()
    xz_copy(z, 0, xw_ref.at[q_rows(y)]).start()
    w_issue(1)
    w_issue(2)
    wp_copy(z, 0, dp, ws_ref.at[z]).start()
    wx_copy(z, 1, dp, ws_ref.at[z]).start()
    wx_copy(z, 0, dp, ws_ref.at[z]).start()

    @pl.loop(1, nz)
    def _(d):
        sq_copy(zmod(z + d), z).start()

    acc[...] = jnp.zeros_like(acc)
    taps_in[0:3] = cg_ref[...]
    taps_in[3:6] = cu_ref[...]
    taps_in[6:8] = jnp.zeros((2, taps_in.shape[1]), F32)
    taps_ref[...] = jnp.transpose(taps_in[...], (1, 0))

    def product(b):
        w_last(b)
        w = wfull[b].reshape(kb, lanes)
        acc[...] += jnp.dot(xfull[b], w, preferred_element_type=F32)

    def with_first(d, fn):
        @pl.when((d >= 2) & (d <= half))
        def _():
            @pl.when(d == 2)
            def _():
                both(1, fn)

            both(d, fn)

    @pl.loop(1, half + 4)
    def _(s):
        @pl.when(s <= half)
        def _():
            br = zmod(z - s)
            xz_copy(br, 1).wait_recv()

            @pl.when(s < half)
            def _():
                xz_copy(br, 1).start()

            x_first(br)

            @pl.when(s < half)
            def _():
                bl = zmod(z + s)
                xz_copy(bl, 0).wait_recv()

                @pl.when(s < half - 1)
                def _():
                    xz_copy(bl, 0).start()

                x_first(bl)

        @pl.when(s + 2 <= half)
        def _():
            w_issue(s + 2)

        @pl.when((s >= 2) & (s <= half + 1))
        def _():
            both(s - 1, x_second)

        with_first(s, w_arrive)

        @pl.when(s == 1)
        def _():
            w_side(z)

        with_first(s - 1, w_side)

        @pl.when(s == 2)
        def _():
            w_far(z)

        with_first(s - 2, w_far)

        @pl.when((s >= 3) & (s <= half + 2))
        def _():
            both(s - 2, x_third)

        @pl.when(s == 3)
        def _():
            product(z)

        with_first(s - 3, product)

    @pl.loop(1, nz)
    def _(d):
        src = zmod(z + d)
        sq_copy(src, src).wait_recv()

    scale = lax.rsqrt(jnp.sum(sq_all[...], axis=0) / dim_full + EPS)
    lin = jnp.transpose(acc[...], (1, 0))
    taps = taps_ref[pl.ds(pl.multiple_of(z * units, units), units), :]

    def conv(field, base):
        lane = lax.broadcasted_iota(jnp.int32, field.shape, 1)
        before = jnp.where(lane == 0, 0.0, pltpu.roll(field, 1, 1))
        after = jnp.where(lane == tokens - 1, 0.0, pltpu.roll(field, tokens - 1, 1))
        return (
            taps[:, base : base + 1] * before
            + taps[:, base + 1 : base + 2] * field
            + taps[:, base + 2 : base + 3] * after
        )

    gate = conv(lin[:units] * scale, 0)
    up = conv(lin[units : 2 * units] * scale, 3)
    hidden = (jax.nn.gelu(gate, approximate=True) * up).astype(BF16)
    hfull[z] = hidden
    step_rows = -(-units // 64) * 16
    cuts = [(r, min(step_rows, units - r)) for r in range(0, units, step_rows)]
    subs = len(cuts)

    def hz_copy(b, c, right):
        ref = hfull.at[b, pl.ds(*cuts[c])]
        return rcopy(ref, ref, hz_s.at[1 - right, b, c], hz_r.at[b, c],
                     {"ra": z_right if right else z_left})

    for c in range(subs):
        hz_copy(z, c, 1).start()
        hz_copy(z, c, 0).start()

    def down(b):
        w = wd_ref[pl.ds(pl.multiple_of(b * units, units), units), :]
        return lax.dot_general(w, hfull[b], (((0,), (0,)), ((), ())), preferred_element_type=F32)

    loads[2].wait()
    part[...] = down(z)

    @pl.loop(1, half)
    def _(s):
        br, bl = zmod(z - s), zmod(z + s)
        for c in range(subs):
            hz_copy(br, c, 1).wait_recv()
            if c < subs // 2:
                hz_copy(br, c, 1).start()
            else:
                @pl.when(s < half - 1)
                def _():
                    hz_copy(br, c, 1).start()
            hz_copy(bl, c, 0).wait_recv()
            if c >= subs // 2:
                hz_copy(bl, c, 0).start()
            else:
                @pl.when(s < half - 1)
                def _():
                    hz_copy(bl, c, 0).start()
        part[...] += down(br)
        part[...] += down(bl)

    far = zmod(z + half)
    for c in range(subs):
        hz_copy(far, c, 1 if c < subs // 2 else 0).wait_recv()
    part[...] += down(far)

    def ps_copy(k, dest):
        return rcopy(psend.at[k], precv.at[k], ps_s.at[k], ps_r.at[k], {"cb": dest})

    def quarter_cols(q):
        return pl.ds(pl.multiple_of(q * quarter, quarter), quarter)

    for k, dest in enumerate((y_far, y_right, y_left)):
        psend[k] = part[:, quarter_cols(dest)].astype(BF16)
        ps_copy(k, dest).start()
    share = part[:, quarter_cols(y)]
    for k, dest in enumerate((y_far, y_right, y_left)):
        ps_copy(k, dest).wait_recv()
        share = share + precv[k].astype(F32)

    def pq_copy(dest, source):
        return rcopy(psq_own, psq_all.at[source], pq_s.at[dest], pq_r.at[source], {"ra": dest})

    own_sq = jnp.sum(share * share, axis=0, keepdims=True)
    psq_own[...] = own_sq
    psq_all[z] = own_sq

    @pl.loop(1, nz)
    def _(d):
        pq_copy(zmod(z + d), z).start()

    branch = jnp.transpose(share, (1, 0)) * gain_ref[...]
    bshare[...] = branch.astype(BF16)

    def mo_copy(k, dest):
        return rcopy(bshare, bfull.at[k], mo_s.at[k], mo_r.at[k], {"cb": dest})

    def po_copy(k, dest):
        return rcopy(post_own, post_all.at[k], po_s.at[k], po_r.at[k], {"cb": dest})

    peers = (y_far, y_right, y_left)
    for k, dest in enumerate(peers):
        mo_copy(k, dest).start()

    @pl.loop(1, nz)
    def _(d):
        src = zmod(z + d)
        pq_copy(src, src).wait_recv()

    post = lax.rsqrt(jnp.sum(psq_all[...], axis=0) / dim_full + EPS)
    post_own[...] = post
    for k, dest in enumerate(peers):
        po_copy(k, dest).start()

    def finish(q, value, scale_row):
        col = jnp.transpose(jnp.broadcast_to(scale_row, (quarter, quarter)), (1, 0))[:, :1]
        base = RESIDUAL * tok_ref[q_rows(q), :].astype(F32)
        out_ref[q_rows(q), :] = (base + value * col).astype(BF16)

    finish(y, branch, post)
    for k, source in enumerate((y_far, y_left, y_right)):
        mo_copy(k, source).wait_recv()
        po_copy(k, source).wait_recv()
        finish(source, bfull[k].astype(F32), post_all[k])

    for c in range(subs):
        first = c < subs // 2

        @pl.loop(0, half)
        def _(t):
            @pl.when(t < (half if first else half - 1))
            def _():
                hz_copy(zmod(z - t), c, 1).wait_send()

            @pl.when(t < (half - 1 if first else half))
            def _():
                hz_copy(zmod(z + t), c, 0).wait_send()

    @pl.loop(0, half)
    def _(t):
        xz_copy(zmod(z - t), 1).wait_send()

        @pl.when(t < half - 1)
        def _():
            xz_copy(zmod(z + t), 0).wait_send()

    @pl.loop(0, nz)
    def _(b):
        @pl.when(b != z)
        def _():
            y1_copy(b, 1, y).wait_send()
            y1_copy(b, 0, y).wait_send()
            y2_copy(b, 1, y_left).wait_send()
            y2_copy(b, 0, y_right).wait_send()
            wz_copy(b, z).wait_send()
            sq_copy(b, z).wait_send()
            pq_copy(b, z).wait_send()

        wx_copy(b, 1, dp).wait_send()
        wx_copy(b, 0, dp).wait_send()
        wo_copy(b, 1, x_left).wait_send()
        for k in range(4):
            wp_copy(b, k, dp).wait_send()

    for k, dest in enumerate(peers):
        ps_copy(k, dest).wait_send()
        mo_copy(k, dest).wait_send()
        po_copy(k, dest).wait_send()


def local(tokens, pre_gain, w_gate, w_up, conv_gate, conv_up, w_down, post_gain):
    nz = lax.axis_size("ra")
    _, positions, kb = tokens.shape
    ff = w_gate.shape[1]
    units = ff // nz
    lanes = -(-2 * units // 128) * 128
    rows = kb // 8
    quarter = positions // 4
    subs = -(-units // (-(-units // 64) * 16))
    dim_full = kb * nz

    dma = pltpu.SemaphoreType.DMA
    vmem = pltpu.VMEM
    scratch = [
        vmem((positions, kb), BF16),
        vmem((1, positions), F32),
        vmem((nz, rows, lanes), BF16),
        vmem((2, rows, ff), BF16),
        vmem((ff, kb), BF16),
        vmem((8, ff), F32),
        vmem((ff, 8), F32),
        vmem((nz, positions, kb), BF16),
        vmem((nz, 8, rows, lanes), BF16),
        vmem((nz, units, positions), BF16),
        vmem((positions, lanes), F32),
        vmem((kb, positions), F32),
        vmem((3, kb, quarter), BF16),
        vmem((3, kb, quarter), BF16),
        vmem((nz, 1, positions), F32),
        vmem((1, quarter), F32),
        vmem((nz, 1, quarter), F32),
        vmem((quarter, kb), BF16),
        vmem((3, quarter, kb), BF16),
        vmem((1, quarter), F32),
        vmem((3, 1, quarter), F32),
        dma((3,)),
        dma((2, nz)), dma((nz,)),
        dma((2, nz)), dma((2, nz)), dma((2, nz)), dma((2, nz)),
        dma((nz,)), dma((nz,)), dma((2, nz)), dma((2, nz)), dma((nz,)), dma((nz,)),
        dma((4, nz)), dma((4, nz)),
        dma((nz,)), dma((nz,)), dma((2, nz, subs)), dma((nz, subs)),
        dma((3,)), dma((3,)), dma((nz,)), dma((nz,)), dma((3,)), dma((3,)), dma((3,)), dma((3,)),
    ]

    here = pl.BlockSpec(memory_space=pltpu.VMEM)
    away = pl.BlockSpec(memory_space=pl.ANY)
    out = pl.pallas_call(
        functools.partial(_kernel, dim_full, nz),
        out_shape=jax.ShapeDtypeStruct((positions, kb), BF16),
        in_specs=[here, here, away, away, here, here, away, here],
        out_specs=pl.BlockSpec(memory_space=pltpu.VMEM),
        scratch_shapes=scratch,
        name="ffn",
        compiler_params=pltpu.CompilerParams(
            collective_id=0, has_side_effects=True, vmem_limit_bytes=48 * 1024 * 1024
        ),
    )(tokens[0], pre_gain[None, :], w_gate, w_up, conv_gate, conv_up, w_down, post_gain[None, :])
    return out[None]


def solution(mesh):
    in_specs = (
        P("dp", None, "ra"),
        P("ra"),
        P("ra", "cb"),
        P("ra", "cb"),
        P(None, "cb"),
        P(None, "cb"),
        P("cb", "ra"),
        P("ra"),
    )
    out_specs = P("dp", None, "ra")
    return jax.shard_map(local, mesh=mesh, in_specs=in_specs, out_specs=out_specs, check_vma=False)
```

```python
import functools
import jax
import jax.numpy as jnp
from jax import lax
from jax.experimental import pallas as pl
from jax.experimental.pallas import tpu as pltpu
from jax.sharding import PartitionSpec as P

EPS = 1e-06
RESIDUAL = 0.125
MESH = pl.DeviceIdType.MESH
BF16 = jnp.bfloat16
F32 = jnp.float32


def _kernel(
    dim_full,
    nz,
    tok_in, pre_in, wg_ref, wu_ref, cg_ref, cu_ref, wd_hbm, gain_in,
    out_ref,
    tok_ref, pre_ref, gain_ref, xw_ref, sq_ref, ws_ref, wrows, wd_ref, taps_g, taps_u, taps_in, taps_ref,
    xfull, wfull, hfull, acc, part, psend, precv, sq_all, psq_own, psq_all,
    bshare, bfull, post_own, post_all, in_sem,
    xz_s, xz_r, y1_s, y1_r, y2_s, y2_r, wz_s, wz_r, wx_s, wx_r, wo_s, wo_r, wp_s, wp_r,
    sq_s, sq_r, hz_s, hz_r, ps_s, ps_r, pq_s, pq_r, mo_s, mo_r, po_s, po_r,
):
    half = nz // 2
    z = lax.axis_index("ra")
    y = lax.axis_index("cb")
    dp = lax.axis_index("dp")
    tokens, kb = xw_ref.shape
    quarter = tokens // 4
    qhalf = quarter // 2
    units = hfull.shape[1]
    rows = wrows.shape[1]
    lanes = acc.shape[1]

    def zmod(v):
        return lax.rem(v + 2 * nz, nz)

    z_right, z_left = zmod(z + 1), zmod(z - 1)
    y_right, y_left, y_far = lax.rem(y + 1, 4), lax.rem(y + 3, 4), lax.rem(y + 2, 4)
    x_right, x_left = lax.rem(dp + 2, 8), lax.rem(dp + 6, 8)
    x_far = lax.rem(dp + 4, 8)
    partner = dp + 1 - 2 * lax.rem(dp, 2)

    def other(v):
        return v + 1 - 2 * lax.rem(v, 2)

    def rcopy(src, dst, ssem, rsem, dev):
        return pltpu.make_async_remote_copy(
            src_ref=src, dst_ref=dst, send_sem=ssem, recv_sem=rsem,
            device_id=dev, device_id_type=MESH,
        )

    bar = pltpu.get_barrier_semaphore()

    @pl.loop(1, nz)
    def _(d):
        pl.semaphore_signal(bar, inc=1, device_id={"ra": zmod(z + d)}, device_id_type=MESH)

    for t in (y_right, y_left, y_far):
        pl.semaphore_signal(bar, inc=1, device_id={"cb": t}, device_id_type=MESH)
    for t in (x_right, x_left, partner):
        pl.semaphore_signal(bar, inc=1, device_id={"dp": t}, device_id_type=MESH)

    own = pl.ds(pl.multiple_of(dp * rows, rows), rows)
    loads = [
        pltpu.make_async_copy(wg_ref.at[own], wrows.at[0], in_sem.at[0]),
        pltpu.make_async_copy(wu_ref.at[own], wrows.at[1], in_sem.at[1]),
        pltpu.make_async_copy(wd_hbm, wd_ref, in_sem.at[2]),
        pltpu.make_async_copy(tok_in, tok_ref, in_sem.at[3]),
        pltpu.make_async_copy(pre_in, pre_ref, in_sem.at[4]),
        pltpu.make_async_copy(gain_in, gain_ref, in_sem.at[5]),
        pltpu.make_async_copy(cg_ref, taps_g, in_sem.at[6]),
        pltpu.make_async_copy(cu_ref, taps_u, in_sem.at[7]),
    ]
    for k in (3, 4, 0, 1, 5, 6, 7, 2):
        loads[k].start()
    loads[3].wait()
    loads[4].wait()
    values = tok_ref[...].astype(F32)
    xw_ref[...] = (values * pre_ref[...]).astype(BF16)
    sq_ref[...] = jnp.sum(jnp.transpose(values * values, (1, 0)), axis=0, keepdims=True)
    loads[0].wait()
    loads[1].wait()
    tail = jnp.zeros((rows, lanes - 2 * units), BF16)
    for j in range(nz):
        cut = slice(j * units, (j + 1) * units)
        ws_ref[j] = jnp.concatenate([wrows[0, :, cut], wrows[1, :, cut], tail], axis=1)
    xfull[z] = xw_ref[...]
    wfull[z, dp] = ws_ref[z]
    sq_all[z] = sq_ref[...]
    pl.semaphore_wait(bar, nz - 1 + 6)

    def q_rows(q):
        return pl.ds(pl.multiple_of(q * quarter, quarter), quarter)

    def qh_rows(q, i):
        return pl.ds(pl.multiple_of(q * quarter + i * qhalf, qhalf), qhalf)

    def xz_copy(b, right, src=None):
        dst = xfull.at[b, q_rows(y)]
        return rcopy(dst if src is None else src, dst, xz_s.at[1 - right, b], xz_r.at[b],
                     {"ra": z_right if right else z_left})

    def y1_copy(b, right, q):
        ref = xfull.at[b, q_rows(q)]
        return rcopy(ref, ref, y1_s.at[1 - right, b], y1_r.at[1 - right, b],
                     {"cb": y_right if right else y_left})

    def y2_copy(b, right, q):
        ref = xfull.at[b, qh_rows(q, 1 - right)]
        return rcopy(ref, ref, y2_s.at[1 - right, b], y2_r.at[1 - right, b],
                     {"cb": y_right if right else y_left})

    def wz_copy(dest, source):
        return rcopy(ws_ref.at[dest], wfull.at[source, dp], wz_s.at[dest], wz_r.at[source],
                     {"ra": dest})

    def wx_copy(b, right, share, src=None):
        ref = wfull.at[b, share]
        return rcopy(ref if src is None else src, ref, wx_s.at[1 - right, b], wx_r.at[1 - right, b],
                     {"dp": x_right if right else x_left})

    def wo_copy(b, right, share):
        ref = wfull.at[b, share]
        return rcopy(ref, ref, wo_s.at[b], wo_r.at[b], {"dp": x_right if right else x_left})

    def wp_copy(b, k, share, src=None):
        ref = wfull.at[b, share]
        return rcopy(ref if src is None else src, ref, wp_s.at[k, b], wp_r.at[k, b], {"dp": partner})

    def sq_copy(dest, source):
        return rcopy(sq_ref, sq_all.at[source], sq_s.at[dest], sq_r.at[source], {"ra": dest})

    def w_issue(d):
        wz_copy(zmod(z + d), z).start()

        @pl.when(d < half)
        def _():
            wz_copy(zmod(z - d), z).start()

    def both(d, fn):
        fn(zmod(z - d))

        @pl.when((d > 0) & (d < half))
        def _():
            fn(zmod(z + d))

    def w_arrive(b):
        wz_copy(b, b).wait_recv()
        wp_copy(b, 0, dp).start()
        wx_copy(b, 1, dp).start()
        wx_copy(b, 0, dp).start()

    def w_side(b):
        wx_copy(b, 1, x_left).wait_recv()
        wx_copy(b, 0, x_right).wait_recv()
        wp_copy(b, 1, x_left).start()
        wp_copy(b, 2, x_right).start()

        @pl.when(lax.rem(b, 2) == 0)
        def _():
            wo_copy(b, 1, x_left).start()

        @pl.when(lax.rem(b, 2) == 1)
        def _():
            wo_copy(b, 0, x_right).start()

    def w_far(b):
        wo_copy(b, 1, x_far).wait_recv()
        wp_copy(b, 3, x_far).start()

    def w_last(b):
        wp_copy(b, 0, partner).wait_recv()
        wp_copy(b, 1, other(x_left)).wait_recv()
        wp_copy(b, 2, other(x_right)).wait_recv()
        wp_copy(b, 3, other(x_far)).wait_recv()

    def x_first(b):
        y1_copy(b, 1, y).start()
        y1_copy(b, 0, y).start()

    def x_second(b):
        y1_copy(b, 1, y_left).wait_recv()
        y2_copy(b, 1, y_left).start()
        y1_copy(b, 0, y_right).wait_recv()
        y2_copy(b, 0, y_right).start()

    def x_third(b):
        y2_copy(b, 1, y_far).wait_recv()
        y2_copy(b, 0, y_far).wait_recv()

    xz_copy(z, 1, xw_ref.at[q_rows(y)]).start()
    xz_copy(z, 0, xw_ref.at[q_rows(y)]).start()
    w_issue(1)
    w_issue(2)
    wp_copy(z, 0, dp, ws_ref.at[z]).start()
    wx_copy(z, 1, dp, ws_ref.at[z]).start()
    wx_copy(z, 0, dp, ws_ref.at[z]).start()

    @pl.loop(1, nz)
    def _(d):
        sq_copy(zmod(z + d), z).start()

    acc[...] = jnp.zeros_like(acc)
    loads[6].wait()
    loads[7].wait()
    taps_in[0:3] = taps_g[...]
    taps_in[3:6] = taps_u[...]
    taps_in[6:8] = jnp.zeros((2, taps_in.shape[1]), F32)
    taps_ref[...] = jnp.transpose(taps_in[...], (1, 0))

    def product(b):
        w_last(b)
        w = wfull[b].reshape(kb, lanes)
        acc[...] += jnp.dot(xfull[b], w, preferred_element_type=F32)

    def with_first(d, fn):
        @pl.when((d >= 2) & (d <= half))
        def _():
            @pl.when(d == 2)
            def _():
                both(1, fn)

            both(d, fn)

    @pl.loop(1, half + 4)
    def _(s):
        @pl.when(s <= half)
        def _():
            br = zmod(z - s)
            xz_copy(br, 1).wait_recv()

            @pl.when(s < half)
            def _():
                xz_copy(br, 1).start()

            x_first(br)

            @pl.when(s < half)
            def _():
                bl = zmod(z + s)
                xz_copy(bl, 0).wait_recv()

                @pl.when(s < half - 1)
                def _():
                    xz_copy(bl, 0).start()

                x_first(bl)

        @pl.when(s + 2 <= half)
        def _():
            w_issue(s + 2)

        @pl.when((s >= 2) & (s <= half + 1))
        def _():
            both(s - 1, x_second)

        with_first(s, w_arrive)

        @pl.when(s == 1)
        def _():
            w_side(z)

        with_first(s - 1, w_side)

        @pl.when(s == 2)
        def _():
            w_far(z)

        with_first(s - 2, w_far)

        @pl.when((s >= 3) & (s <= half + 2))
        def _():
            both(s - 2, x_third)

        @pl.when(s == 3)
        def _():
            product(z)

        with_first(s - 3, product)

    @pl.loop(1, nz)
    def _(d):
        src = zmod(z + d)
        sq_copy(src, src).wait_recv()

    scale = lax.rsqrt(jnp.sum(sq_all[...], axis=0) / dim_full + EPS)
    lin = jnp.transpose(acc[...], (1, 0))
    taps = taps_ref[pl.ds(pl.multiple_of(z * units, units), units), :]

    def conv(field, base):
        lane = lax.broadcasted_iota(jnp.int32, field.shape, 1)
        before = jnp.where(lane == 0, 0.0, pltpu.roll(field, 1, 1))
        after = jnp.where(lane == tokens - 1, 0.0, pltpu.roll(field, tokens - 1, 1))
        return (
            taps[:, base : base + 1] * before
            + taps[:, base + 1 : base + 2] * field
            + taps[:, base + 2 : base + 3] * after
        )

    gate = conv(lin[:units] * scale, 0)
    up = conv(lin[units : 2 * units] * scale, 3)
    hidden = (jax.nn.gelu(gate, approximate=True) * up).astype(BF16)
    hfull[z] = hidden
    step_rows = -(-units // 64) * 16
    cuts = [(r, min(step_rows, units - r)) for r in range(0, units, step_rows)]
    subs = len(cuts)

    def hz_copy(b, c, right):
        ref = hfull.at[b, pl.ds(*cuts[c])]
        return rcopy(ref, ref, hz_s.at[1 - right, b, c], hz_r.at[b, c],
                     {"ra": z_right if right else z_left})

    for c in range(subs):
        hz_copy(z, c, 1).start()
        hz_copy(z, c, 0).start()

    def down(b):
        w = wd_ref[pl.ds(pl.multiple_of(b * units, units), units), :]
        return lax.dot_general(w, hfull[b], (((0,), (0,)), ((), ())), preferred_element_type=F32)

    loads[2].wait()
    loads[5].wait()
    part[...] = down(z)

    @pl.loop(1, half)
    def _(s):
        br, bl = zmod(z - s), zmod(z + s)
        for c in range(subs):
            hz_copy(br, c, 1).wait_recv()
            if c < subs // 2:
                hz_copy(br, c, 1).start()
            else:
                @pl.when(s < half - 1)
                def _():
                    hz_copy(br, c, 1).start()
            hz_copy(bl, c, 0).wait_recv()
            if c >= subs // 2:
                hz_copy(bl, c, 0).start()
            else:
                @pl.when(s < half - 1)
                def _():
                    hz_copy(bl, c, 0).start()
        part[...] += down(br)
        part[...] += down(bl)

    far = zmod(z + half)
    for c in range(subs):
        hz_copy(far, c, 1 if c < subs // 2 else 0).wait_recv()
    part[...] += down(far)

    def ps_copy(k, dest):
        return rcopy(psend.at[k], precv.at[k], ps_s.at[k], ps_r.at[k], {"cb": dest})

    def quarter_cols(q):
        return pl.ds(pl.multiple_of(q * quarter, quarter), quarter)

    for k, dest in enumerate((y_far, y_right, y_left)):
        psend[k] = part[:, quarter_cols(dest)].astype(BF16)
        ps_copy(k, dest).start()
    share = part[:, quarter_cols(y)]
    for k, dest in enumerate((y_far, y_right, y_left)):
        ps_copy(k, dest).wait_recv()
        share = share + precv[k].astype(F32)

    def pq_copy(dest, source):
        return rcopy(psq_own, psq_all.at[source], pq_s.at[dest], pq_r.at[source], {"ra": dest})

    own_sq = jnp.sum(share * share, axis=0, keepdims=True)
    psq_own[...] = own_sq
    psq_all[z] = own_sq

    @pl.loop(1, nz)
    def _(d):
        pq_copy(zmod(z + d), z).start()

    branch = jnp.transpose(share, (1, 0)) * gain_ref[...]
    bshare[...] = branch.astype(BF16)

    def mo_copy(k, dest):
        return rcopy(bshare, bfull.at[k], mo_s.at[k], mo_r.at[k], {"cb": dest})

    def po_copy(k, dest):
        return rcopy(post_own, post_all.at[k], po_s.at[k], po_r.at[k], {"cb": dest})

    peers = (y_far, y_right, y_left)
    for k, dest in enumerate(peers):
        mo_copy(k, dest).start()

    @pl.loop(1, nz)
    def _(d):
        src = zmod(z + d)
        pq_copy(src, src).wait_recv()

    post = lax.rsqrt(jnp.sum(psq_all[...], axis=0) / dim_full + EPS)
    post_own[...] = post
    for k, dest in enumerate(peers):
        po_copy(k, dest).start()

    def finish(q, value, scale_row):
        col = jnp.transpose(jnp.broadcast_to(scale_row, (quarter, quarter)), (1, 0))[:, :1]
        base = RESIDUAL * tok_ref[q_rows(q), :].astype(F32)
        out_ref[q_rows(q), :] = (base + value * col).astype(BF16)

    finish(y, branch, post)
    for k, source in enumerate((y_far, y_left, y_right)):
        mo_copy(k, source).wait_recv()
        po_copy(k, source).wait_recv()
        finish(source, bfull[k].astype(F32), post_all[k])

    for c in range(subs):
        first = c < subs // 2

        @pl.loop(0, half)
        def _(t):
            @pl.when(t < (half if first else half - 1))
            def _():
                hz_copy(zmod(z - t), c, 1).wait_send()

            @pl.when(t < (half - 1 if first else half))
            def _():
                hz_copy(zmod(z + t), c, 0).wait_send()

    @pl.loop(0, half)
    def _(t):
        xz_copy(zmod(z - t), 1).wait_send()

        @pl.when(t < half - 1)
        def _():
            xz_copy(zmod(z + t), 0).wait_send()

    @pl.loop(0, nz)
    def _(b):
        @pl.when(b != z)
        def _():
            y1_copy(b, 1, y).wait_send()
            y1_copy(b, 0, y).wait_send()
            y2_copy(b, 1, y_left).wait_send()
            y2_copy(b, 0, y_right).wait_send()
            wz_copy(b, z).wait_send()
            sq_copy(b, z).wait_send()
            pq_copy(b, z).wait_send()

        wx_copy(b, 1, dp).wait_send()
        wx_copy(b, 0, dp).wait_send()
        wo_copy(b, 1, x_left).wait_send()
        for k in range(4):
            wp_copy(b, k, dp).wait_send()

    for k, dest in enumerate(peers):
        ps_copy(k, dest).wait_send()
        mo_copy(k, dest).wait_send()
        po_copy(k, dest).wait_send()


def local(tokens, pre_gain, w_gate, w_up, conv_gate, conv_up, w_down, post_gain):
    nz = lax.axis_size("ra")
    _, positions, kb = tokens.shape
    ff = w_gate.shape[1]
    units = ff // nz
    lanes = -(-2 * units // 128) * 128
    rows = kb // 8
    quarter = positions // 4
    subs = -(-units // (-(-units // 64) * 16))
    dim_full = kb * nz

    dma = pltpu.SemaphoreType.DMA
    vmem = pltpu.VMEM
    scratch = [
        vmem((positions, kb), BF16),
        vmem((1, kb), F32),
        vmem((1, kb), F32),
        vmem((positions, kb), BF16),
        vmem((1, positions), F32),
        vmem((nz, rows, lanes), BF16),
        vmem((2, rows, ff), BF16),
        vmem((ff, kb), BF16),
        vmem((3, ff), F32),
        vmem((3, ff), F32),
        vmem((8, ff), F32),
        vmem((ff, 8), F32),
        vmem((nz, positions, kb), BF16),
        vmem((nz, 8, rows, lanes), BF16),
        vmem((nz, units, positions), BF16),
        vmem((positions, lanes), F32),
        vmem((kb, positions), F32),
        vmem((3, kb, quarter), BF16),
        vmem((3, kb, quarter), BF16),
        vmem((nz, 1, positions), F32),
        vmem((1, quarter), F32),
        vmem((nz, 1, quarter), F32),
        vmem((quarter, kb), BF16),
        vmem((3, quarter, kb), BF16),
        vmem((1, quarter), F32),
        vmem((3, 1, quarter), F32),
        dma((8,)),
        dma((2, nz)), dma((nz,)),
        dma((2, nz)), dma((2, nz)), dma((2, nz)), dma((2, nz)),
        dma((nz,)), dma((nz,)), dma((2, nz)), dma((2, nz)), dma((nz,)), dma((nz,)),
        dma((4, nz)), dma((4, nz)),
        dma((nz,)), dma((nz,)), dma((2, nz, subs)), dma((nz, subs)),
        dma((3,)), dma((3,)), dma((nz,)), dma((nz,)), dma((3,)), dma((3,)), dma((3,)), dma((3,)),
    ]

    here = pl.BlockSpec(memory_space=pltpu.VMEM)
    away = pl.BlockSpec(memory_space=pl.ANY)
    out = pl.pallas_call(
        functools.partial(_kernel, dim_full, nz),
        out_shape=jax.ShapeDtypeStruct((positions, kb), BF16),
        in_specs=[away] * 8,
        out_specs=pl.BlockSpec(memory_space=pltpu.VMEM),
        scratch_shapes=scratch,
        name="ffn",
        compiler_params=pltpu.CompilerParams(
            collective_id=0, has_side_effects=True, vmem_limit_bytes=67043328
        ),
    )(tokens[0], pre_gain[None, :], w_gate, w_up, conv_gate, conv_up, w_down, post_gain[None, :])
    return out[None]


def solution(mesh):
    in_specs = (
        P("dp", None, "ra"),
        P("ra"),
        P("ra", "cb"),
        P("ra", "cb"),
        P(None, "cb"),
        P(None, "cb"),
        P("cb", "ra"),
        P("ra"),
    )
    out_specs = P("dp", None, "ra")
    return jax.shard_map(local, mesh=mesh, in_specs=in_specs, out_specs=out_specs, check_vma=False)
```

```python
import functools
import jax
import jax.numpy as jnp
from jax import lax
from jax.experimental import pallas as pl
from jax.experimental.pallas import tpu as pltpu
from jax.sharding import PartitionSpec as P

EPS = 1e-06
RESIDUAL = 0.125
MESH = pl.DeviceIdType.MESH
BF16 = jnp.bfloat16
F32 = jnp.float32


def _kernel(
    dim_full,
    nz,
    tok_in, pre_in, wg_ref, wu_ref, cg_ref, cu_ref, wd_hbm, gain_in,
    out_ref,
    tok_ref, pre_ref, gain_ref, xw_ref, sq_ref, ws_ref, wrows, wd_ref, taps_g, taps_u, taps_in, taps_ref,
    xfull, wfull, hfull, acc, lin, part, psend, precv, sq_all, psq_own, psq_all,
    bshare, bfull, post_own, post_all, in_sem,
    xz_s, xz_r, y1_s, y1_r, y2_s, y2_r, wz_s, wz_r, wx_s, wx_r, wo_s, wo_r, wp_s, wp_r,
    sq_s, sq_r, hz_s, hz_r, ps_s, ps_r, pq_s, pq_r, mo_s, mo_r, po_s, po_r,
):
    half = nz // 2
    z = lax.axis_index("ra")
    y = lax.axis_index("cb")
    dp = lax.axis_index("dp")
    tokens, kb = xw_ref.shape
    quarter = tokens // 4
    qhalf = quarter // 2
    units = hfull.shape[1]
    rows = wrows.shape[1]
    lanes = acc.shape[1]

    def zmod(v):
        return lax.rem(v + 2 * nz, nz)

    z_right, z_left = zmod(z + 1), zmod(z - 1)
    y_right, y_left, y_far = lax.rem(y + 1, 4), lax.rem(y + 3, 4), lax.rem(y + 2, 4)
    x_right, x_left = lax.rem(dp + 2, 8), lax.rem(dp + 6, 8)
    x_far = lax.rem(dp + 4, 8)
    partner = dp + 1 - 2 * lax.rem(dp, 2)

    def other(v):
        return v + 1 - 2 * lax.rem(v, 2)

    def rcopy(src, dst, ssem, rsem, dev):
        return pltpu.make_async_remote_copy(
            src_ref=src, dst_ref=dst, send_sem=ssem, recv_sem=rsem,
            device_id=dev, device_id_type=MESH,
        )

    bar = pltpu.get_barrier_semaphore()

    @pl.loop(1, nz)
    def _(d):
        pl.semaphore_signal(bar, inc=1, device_id={"ra": zmod(z + d)}, device_id_type=MESH)

    for t in (y_right, y_left, y_far):
        pl.semaphore_signal(bar, inc=1, device_id={"cb": t}, device_id_type=MESH)
    for t in (x_right, x_left, partner):
        pl.semaphore_signal(bar, inc=1, device_id={"dp": t}, device_id_type=MESH)

    own = pl.ds(pl.multiple_of(dp * rows, rows), rows)
    loads = [
        pltpu.make_async_copy(wg_ref.at[own], wrows.at[0], in_sem.at[0]),
        pltpu.make_async_copy(wu_ref.at[own], wrows.at[1], in_sem.at[1]),
        pltpu.make_async_copy(wd_hbm, wd_ref, in_sem.at[2]),
        pltpu.make_async_copy(tok_in, tok_ref, in_sem.at[3]),
        pltpu.make_async_copy(pre_in, pre_ref, in_sem.at[4]),
        pltpu.make_async_copy(gain_in, gain_ref, in_sem.at[5]),
        pltpu.make_async_copy(cg_ref, taps_g, in_sem.at[6]),
        pltpu.make_async_copy(cu_ref, taps_u, in_sem.at[7]),
    ]
    for k in (3, 4, 0, 1, 5, 6, 7, 2):
        loads[k].start()
    loads[3].wait()
    loads[4].wait()
    values = tok_ref[...].astype(F32)
    xw_ref[...] = (values * pre_ref[...]).astype(BF16)
    sq_ref[...] = jnp.sum(jnp.transpose(values * values, (1, 0)), axis=0, keepdims=True)
    loads[0].wait()
    loads[1].wait()
    tail = jnp.zeros((rows, lanes - 2 * units), BF16)
    for j in range(nz):
        cut = slice(j * units, (j + 1) * units)
        ws_ref[j] = jnp.concatenate([wrows[0, :, cut], wrows[1, :, cut], tail], axis=1)
    xfull[z] = xw_ref[...]
    wfull[z, dp] = ws_ref[z]
    sq_all[z] = sq_ref[...]
    pl.semaphore_wait(bar, nz - 1 + 6)

    def q_rows(q):
        return pl.ds(pl.multiple_of(q * quarter, quarter), quarter)

    def qh_rows(q, i):
        return pl.ds(pl.multiple_of(q * quarter + i * qhalf, qhalf), qhalf)

    def xz_copy(b, right, src=None):
        dst = xfull.at[b, q_rows(y)]
        return rcopy(dst if src is None else src, dst, xz_s.at[1 - right, b], xz_r.at[b],
                     {"ra": z_right if right else z_left})

    def y1_copy(b, right, q):
        ref = xfull.at[b, q_rows(q)]
        return rcopy(ref, ref, y1_s.at[1 - right, b], y1_r.at[1 - right, b],
                     {"cb": y_right if right else y_left})

    def y2_copy(b, right, q):
        ref = xfull.at[b, qh_rows(q, 1 - right)]
        return rcopy(ref, ref, y2_s.at[1 - right, b], y2_r.at[1 - right, b],
                     {"cb": y_right if right else y_left})

    def wz_copy(dest, source):
        return rcopy(ws_ref.at[dest], wfull.at[source, dp], wz_s.at[dest], wz_r.at[source],
                     {"ra": dest})

    def wx_copy(b, right, share, src=None):
        ref = wfull.at[b, share]
        return rcopy(ref if src is None else src, ref, wx_s.at[1 - right, b], wx_r.at[1 - right, b],
                     {"dp": x_right if right else x_left})

    def wo_copy(b, right, share):
        ref = wfull.at[b, share]
        return rcopy(ref, ref, wo_s.at[b], wo_r.at[b], {"dp": x_right if right else x_left})

    def wp_copy(b, k, share, src=None):
        ref = wfull.at[b, share]
        return rcopy(ref if src is None else src, ref, wp_s.at[k, b], wp_r.at[k, b], {"dp": partner})

    def sq_copy(dest, source):
        return rcopy(sq_ref, sq_all.at[source], sq_s.at[dest], sq_r.at[source], {"ra": dest})

    def w_issue(d):
        wz_copy(zmod(z + d), z).start()

        @pl.when(d < half)
        def _():
            wz_copy(zmod(z - d), z).start()

    def both(d, fn):
        fn(zmod(z - d))

        @pl.when((d > 0) & (d < half))
        def _():
            fn(zmod(z + d))

    def w_arrive(b):
        wz_copy(b, b).wait_recv()
        wp_copy(b, 0, dp).start()
        wx_copy(b, 1, dp).start()
        wx_copy(b, 0, dp).start()

    def w_side(b):
        wx_copy(b, 1, x_left).wait_recv()
        wx_copy(b, 0, x_right).wait_recv()
        wp_copy(b, 1, x_left).start()
        wp_copy(b, 2, x_right).start()

        @pl.when(lax.rem(b, 2) == 0)
        def _():
            wo_copy(b, 1, x_left).start()

        @pl.when(lax.rem(b, 2) == 1)
        def _():
            wo_copy(b, 0, x_right).start()

    def w_far(b):
        wo_copy(b, 1, x_far).wait_recv()
        wp_copy(b, 3, x_far).start()

    def w_last(b):
        wp_copy(b, 0, partner).wait_recv()
        wp_copy(b, 1, other(x_left)).wait_recv()
        wp_copy(b, 2, other(x_right)).wait_recv()
        wp_copy(b, 3, other(x_far)).wait_recv()

    def x_first(b):
        y1_copy(b, 1, y).start()
        y1_copy(b, 0, y).start()

    def x_second(b):
        y1_copy(b, 1, y_left).wait_recv()
        y2_copy(b, 1, y_left).start()
        y1_copy(b, 0, y_right).wait_recv()
        y2_copy(b, 0, y_right).start()

    def x_third(b):
        y2_copy(b, 1, y_far).wait_recv()
        y2_copy(b, 0, y_far).wait_recv()

    xz_copy(z, 1, xw_ref.at[q_rows(y)]).start()
    xz_copy(z, 0, xw_ref.at[q_rows(y)]).start()
    w_issue(1)
    w_issue(2)
    wp_copy(z, 0, dp, ws_ref.at[z]).start()
    wx_copy(z, 1, dp, ws_ref.at[z]).start()
    wx_copy(z, 0, dp, ws_ref.at[z]).start()

    @pl.loop(1, nz)
    def _(d):
        sq_copy(zmod(z + d), z).start()

    acc[...] = jnp.zeros_like(acc)
    loads[6].wait()
    loads[7].wait()
    taps_in[0:3] = taps_g[...]
    taps_in[3:6] = taps_u[...]
    taps_in[6:8] = jnp.zeros((2, taps_in.shape[1]), F32)
    taps_ref[...] = jnp.transpose(taps_in[...], (1, 0))

    def product(b):
        w_last(b)
        w = wfull[b].reshape(kb, lanes)
        acc[...] += jnp.dot(xfull[b], w, preferred_element_type=F32)

    def with_first(d, fn):
        @pl.when((d >= 2) & (d <= half))
        def _():
            @pl.when(d == 2)
            def _():
                both(1, fn)

            both(d, fn)

    @pl.loop(1, half + 4)
    def _(s):
        @pl.when(s <= half)
        def _():
            br = zmod(z - s)
            xz_copy(br, 1).wait_recv()

            @pl.when(s < half)
            def _():
                xz_copy(br, 1).start()

            x_first(br)

            @pl.when(s < half)
            def _():
                bl = zmod(z + s)
                xz_copy(bl, 0).wait_recv()

                @pl.when(s < half - 1)
                def _():
                    xz_copy(bl, 0).start()

                x_first(bl)

        @pl.when(s + 2 <= half)
        def _():
            w_issue(s + 2)

        @pl.when((s >= 2) & (s <= half + 1))
        def _():
            both(s - 1, x_second)

        with_first(s, w_arrive)

        @pl.when(s == 1)
        def _():
            w_side(z)

        with_first(s - 1, w_side)

        @pl.when(s == 2)
        def _():
            w_far(z)

        with_first(s - 2, w_far)

        @pl.when((s >= 3) & (s <= half + 2))
        def _():
            both(s - 2, x_third)

        @pl.when(s == 3)
        def _():
            product(z)

        with_first(s - 3, product)

    @pl.loop(1, nz)
    def _(d):
        src = zmod(z + d)
        sq_copy(src, src).wait_recv()

    scale = lax.rsqrt(jnp.sum(sq_all[...], axis=0) / dim_full + EPS)
    lin[...] = jnp.transpose(acc[...], (1, 0))
    step_rows = -(-units // 64) * 16
    cuts = [(r, min(step_rows, units - r)) for r in range(0, units, step_rows)]
    subs = len(cuts)

    def hz_copy(b, c, right):
        ref = hfull.at[b, pl.ds(*cuts[c])]
        return rcopy(ref, ref, hz_s.at[1 - right, b, c], hz_r.at[b, c],
                     {"ra": z_right if right else z_left})

    def conv(field, taps, base):
        lane = lax.broadcasted_iota(jnp.int32, field.shape, 1)
        before = jnp.where(lane == 0, 0.0, pltpu.roll(field, 1, 1))
        after = jnp.where(lane == tokens - 1, 0.0, pltpu.roll(field, tokens - 1, 1))
        return (
            taps[:, base : base + 1] * before
            + taps[:, base + 1 : base + 2] * field
            + taps[:, base + 2 : base + 3] * after
        )

    for c, (r, count) in enumerate(cuts):
        taps = taps_ref[pl.ds(pl.multiple_of(z * units + r, 16), count), :]
        gate = conv(lin[r : r + count] * scale, taps, 0)
        up = conv(lin[units + r : units + r + count] * scale, taps, 3)
        hfull[z, r : r + count] = (jax.nn.gelu(gate, approximate=True) * up).astype(BF16)
        hz_copy(z, c, 1).start()
        hz_copy(z, c, 0).start()

    def drain_first(b):
        wx_copy(b, 1, dp).wait_send()
        wx_copy(b, 0, dp).wait_send()
        wo_copy(b, 1, x_left).wait_send()
        for k in range(4):
            wp_copy(b, k, dp).wait_send()

        @pl.when(b != z)
        def _():
            y1_copy(b, 1, y).wait_send()
            y1_copy(b, 0, y).wait_send()
            y2_copy(b, 1, y_left).wait_send()
            y2_copy(b, 0, y_right).wait_send()
            wz_copy(b, z).wait_send()
            sq_copy(b, z).wait_send()

    def down(b):
        w = wd_ref[pl.ds(pl.multiple_of(b * units, units), units), :]
        return lax.dot_general(w, hfull[b], (((0,), (0,)), ((), ())), preferred_element_type=F32)

    loads[2].wait()
    loads[5].wait()
    part[...] = down(z)

    @pl.loop(1, half)
    def _(s):
        br, bl = zmod(z - s), zmod(z + s)
        for c in range(subs):
            hz_copy(br, c, 1).wait_recv()
            if c < subs // 2:
                hz_copy(br, c, 1).start()
            else:
                @pl.when(s < half - 1)
                def _():
                    hz_copy(br, c, 1).start()
            hz_copy(bl, c, 0).wait_recv()
            if c >= subs // 2:
                hz_copy(bl, c, 0).start()
            else:
                @pl.when(s < half - 1)
                def _():
                    hz_copy(bl, c, 0).start()
        part[...] += down(br)
        part[...] += down(bl)
        drain_first(br)
        drain_first(bl)

    far = zmod(z + half)
    for c in range(subs):
        hz_copy(far, c, 1 if c < subs // 2 else 0).wait_recv()
    part[...] += down(far)

    def ps_copy(k, dest):
        return rcopy(psend.at[k], precv.at[k], ps_s.at[k], ps_r.at[k], {"cb": dest})

    def quarter_cols(q):
        return pl.ds(pl.multiple_of(q * quarter, quarter), quarter)

    for k, dest in enumerate((y_far, y_right, y_left)):
        psend[k] = part[:, quarter_cols(dest)].astype(BF16)
        ps_copy(k, dest).start()

    for c in range(subs):
        first = c < subs // 2

        @pl.loop(0, half)
        def _(t):
            @pl.when(t < (half if first else half - 1))
            def _():
                hz_copy(zmod(z - t), c, 1).wait_send()

            @pl.when(t < (half - 1 if first else half))
            def _():
                hz_copy(zmod(z + t), c, 0).wait_send()

    @pl.loop(0, half)
    def _(t):
        xz_copy(zmod(z - t), 1).wait_send()

        @pl.when(t < half - 1)
        def _():
            xz_copy(zmod(z + t), 0).wait_send()

    drain_first(z)
    drain_first(far)
    share = part[:, quarter_cols(y)]
    for k, dest in enumerate((y_far, y_right, y_left)):
        ps_copy(k, dest).wait_recv()
        share = share + precv[k].astype(F32)

    def pq_copy(dest, source):
        return rcopy(psq_own, psq_all.at[source], pq_s.at[dest], pq_r.at[source], {"ra": dest})

    own_sq = jnp.sum(share * share, axis=0, keepdims=True)
    psq_own[...] = own_sq
    psq_all[z] = own_sq

    @pl.loop(1, nz)
    def _(d):
        pq_copy(zmod(z + d), z).start()

    branch = jnp.transpose(share, (1, 0)) * gain_ref[...]
    bshare[...] = branch.astype(BF16)

    def mo_copy(k, dest):
        return rcopy(bshare, bfull.at[k], mo_s.at[k], mo_r.at[k], {"cb": dest})

    def po_copy(k, dest):
        return rcopy(post_own, post_all.at[k], po_s.at[k], po_r.at[k], {"cb": dest})

    peers = (y_far, y_right, y_left)
    for k, dest in enumerate(peers):
        mo_copy(k, dest).start()

    @pl.loop(1, nz)
    def _(d):
        src = zmod(z + d)
        pq_copy(src, src).wait_recv()

    post = lax.rsqrt(jnp.sum(psq_all[...], axis=0) / dim_full + EPS)
    post_own[...] = post
    for k, dest in enumerate(peers):
        po_copy(k, dest).start()

    def finish(q, value, scale_row):
        col = jnp.transpose(jnp.broadcast_to(scale_row, (quarter, quarter)), (1, 0))[:, :1]
        base = RESIDUAL * tok_ref[q_rows(q), :].astype(F32)
        out_ref[q_rows(q), :] = (base + value * col).astype(BF16)

    for k, dest in enumerate(peers):
        ps_copy(k, dest).wait_send()

    @pl.loop(1, nz)
    def _(d):
        pq_copy(zmod(z + d), z).wait_send()

    finish(y, branch, post)
    for k, source in enumerate((y_far, y_left, y_right)):
        mo_copy(k, source).wait_recv()
        po_copy(k, source).wait_recv()
        finish(source, bfull[k].astype(F32), post_all[k])

    for k, dest in enumerate(peers):
        mo_copy(k, dest).wait_send()
        po_copy(k, dest).wait_send()


def local(tokens, pre_gain, w_gate, w_up, conv_gate, conv_up, w_down, post_gain):
    nz = lax.axis_size("ra")
    _, positions, kb = tokens.shape
    ff = w_gate.shape[1]
    units = ff // nz
    lanes = -(-2 * units // 128) * 128
    rows = kb // 8
    quarter = positions // 4
    subs = -(-units // (-(-units // 64) * 16))
    dim_full = kb * nz

    dma = pltpu.SemaphoreType.DMA
    vmem = pltpu.VMEM
    scratch = [
        vmem((positions, kb), BF16),
        vmem((1, kb), F32),
        vmem((1, kb), F32),
        vmem((positions, kb), BF16),
        vmem((1, positions), F32),
        vmem((nz, rows, lanes), BF16),
        vmem((2, rows, ff), BF16),
        vmem((ff, kb), BF16),
        vmem((3, ff), F32),
        vmem((3, ff), F32),
        vmem((8, ff), F32),
        vmem((ff, 8), F32),
        vmem((nz, positions, kb), BF16),
        vmem((nz, 8, rows, lanes), BF16),
        vmem((nz, units, positions), BF16),
        vmem((positions, lanes), F32),
        vmem((lanes, positions), F32),
        vmem((kb, positions), F32),
        vmem((3, kb, quarter), BF16),
        vmem((3, kb, quarter), BF16),
        vmem((nz, 1, positions), F32),
        vmem((1, quarter), F32),
        vmem((nz, 1, quarter), F32),
        vmem((quarter, kb), BF16),
        vmem((3, quarter, kb), BF16),
        vmem((1, quarter), F32),
        vmem((3, 1, quarter), F32),
        dma((8,)),
        dma((2, nz)), dma((nz,)),
        dma((2, nz)), dma((2, nz)), dma((2, nz)), dma((2, nz)),
        dma((nz,)), dma((nz,)), dma((2, nz)), dma((2, nz)), dma((nz,)), dma((nz,)),
        dma((4, nz)), dma((4, nz)),
        dma((nz,)), dma((nz,)), dma((2, nz, subs)), dma((nz, subs)),
        dma((3,)), dma((3,)), dma((nz,)), dma((nz,)), dma((3,)), dma((3,)), dma((3,)), dma((3,)),
    ]

    here = pl.BlockSpec(memory_space=pltpu.VMEM)
    away = pl.BlockSpec(memory_space=pl.ANY)
    out = pl.pallas_call(
        functools.partial(_kernel, dim_full, nz),
        out_shape=jax.ShapeDtypeStruct((positions, kb), BF16),
        in_specs=[away] * 8,
        out_specs=pl.BlockSpec(memory_space=pltpu.VMEM),
        scratch_shapes=scratch,
        name="ffn",
        compiler_params=pltpu.CompilerParams(
            collective_id=0, has_side_effects=True, vmem_limit_bytes=67043328
        ),
    )(tokens[0], pre_gain[None, :], w_gate, w_up, conv_gate, conv_up, w_down, post_gain[None, :])
    return out[None]


def solution(mesh):
    in_specs = (
        P("dp", None, "ra"),
        P("ra"),
        P("ra", "cb"),
        P("ra", "cb"),
        P(None, "cb"),
        P(None, "cb"),
        P("cb", "ra"),
        P("ra"),
    )
    out_specs = P("dp", None, "ra")
    return jax.shard_map(local, mesh=mesh, in_specs=in_specs, out_specs=out_specs, check_vma=False)
```

```python
import functools
import jax
import jax.numpy as jnp
from jax import lax
from jax.experimental import pallas as pl
from jax.experimental.pallas import tpu as pltpu
from jax.sharding import PartitionSpec as P

EPS = 1e-06
RESIDUAL = 0.125
MESH = pl.DeviceIdType.MESH
BF16 = jnp.bfloat16
F32 = jnp.float32


def _kernel(
    dim_full,
    nz,
    tok_in, pre_in, wg_ref, wu_ref, cg_ref, cu_ref, wd_hbm, gain_in,
    out_ref,
    tok_ref, pre_ref, gain_ref, xw_ref, sq_ref, ws_ref, wrows, wd_ref, taps_g, taps_u, taps_in, taps_ref,
    xfull, wfull, hfull, acc, lin, part, psend, precv, sq_all, psq_own, psq_all,
    bshare, bfull, post_own, post_all, in_sem,
    xz_s, xz_r, y1_s, y1_r, y2_s, y2_r, wz_s, wz_r, wx_s, wx_r, wo_s, wo_r, wp_s, wp_r,
    sq_s, sq_r, hz_s, hz_r, ps_s, ps_r, pq_s, pq_r, mo_s, mo_r, po_s, po_r, in_right, in_left,
):
    half = nz // 2
    z = lax.axis_index("ra")
    y = lax.axis_index("cb")
    dp = lax.axis_index("dp")
    tokens, kb = xw_ref.shape
    quarter = tokens // 4
    qhalf = quarter // 2
    units = hfull.shape[1]
    rows = wrows.shape[1]
    lanes = acc.shape[1]

    def zmod(v):
        return lax.rem(v + 2 * nz, nz)

    z_right, z_left = zmod(z + 1), zmod(z - 1)
    y_right, y_left, y_far = lax.rem(y + 1, 4), lax.rem(y + 3, 4), lax.rem(y + 2, 4)
    x_right, x_left = lax.rem(dp + 2, 8), lax.rem(dp + 6, 8)
    x_far = lax.rem(dp + 4, 8)
    partner = dp + 1 - 2 * lax.rem(dp, 2)

    def other(v):
        return v + 1 - 2 * lax.rem(v, 2)

    def rcopy(src, dst, ssem, rsem, dev):
        return pltpu.make_async_remote_copy(
            src_ref=src, dst_ref=dst, send_sem=ssem, recv_sem=rsem,
            device_id=dev, device_id_type=MESH,
        )

    bar = pltpu.get_barrier_semaphore()

    for t in (z_right, z_left):
        pl.semaphore_signal(bar, inc=1, device_id={"ra": t}, device_id_type=MESH)
    for t in (y_right, y_left, y_far):
        pl.semaphore_signal(bar, inc=1, device_id={"cb": t}, device_id_type=MESH)
    for t in (x_right, x_left, partner):
        pl.semaphore_signal(bar, inc=1, device_id={"dp": t}, device_id_type=MESH)

    own = pl.ds(pl.multiple_of(dp * rows, rows), rows)
    loads = [
        pltpu.make_async_copy(wg_ref.at[own], wrows.at[0], in_sem.at[0]),
        pltpu.make_async_copy(wu_ref.at[own], wrows.at[1], in_sem.at[1]),
        pltpu.make_async_copy(wd_hbm, wd_ref, in_sem.at[2]),
        pltpu.make_async_copy(tok_in, tok_ref, in_sem.at[3]),
        pltpu.make_async_copy(pre_in, pre_ref, in_sem.at[4]),
        pltpu.make_async_copy(gain_in, gain_ref, in_sem.at[5]),
        pltpu.make_async_copy(cg_ref, taps_g, in_sem.at[6]),
        pltpu.make_async_copy(cu_ref, taps_u, in_sem.at[7]),
    ]
    for k in (3, 4, 0, 1, 5, 6, 7, 2):
        loads[k].start()
    loads[3].wait()
    loads[4].wait()
    values = tok_ref[...].astype(F32)
    xw_ref[...] = (values * pre_ref[...]).astype(BF16)
    pl.semaphore_wait(bar, 8)

    def relay(k):
        @pl.when(k <= half)
        def _():
            pl.semaphore_signal(in_right, inc=1, device_id={"ra": z_right}, device_id_type=MESH)

        @pl.when(k < half)
        def _():
            pl.semaphore_signal(in_left, inc=1, device_id={"ra": z_left}, device_id_type=MESH)

    def heard(k):
        @pl.when(k <= half)
        def _():
            pl.semaphore_wait(in_right, 1)

        @pl.when(k < half)
        def _():
            pl.semaphore_wait(in_left, 1)

        relay(k + 1)

    relay(2)

    def q_rows(q):
        return pl.ds(pl.multiple_of(q * quarter, quarter), quarter)

    def qh_rows(q, i):
        return pl.ds(pl.multiple_of(q * quarter + i * qhalf, qhalf), qhalf)

    def xz_copy(b, right, src=None):
        dst = xfull.at[b, q_rows(y)]
        return rcopy(dst if src is None else src, dst, xz_s.at[1 - right, b], xz_r.at[b],
                     {"ra": z_right if right else z_left})

    def y1_copy(b, right, q):
        ref = xfull.at[b, q_rows(q)]
        return rcopy(ref, ref, y1_s.at[1 - right, b], y1_r.at[1 - right, b],
                     {"cb": y_right if right else y_left})

    def y2_copy(b, right, q):
        ref = xfull.at[b, qh_rows(q, 1 - right)]
        return rcopy(ref, ref, y2_s.at[1 - right, b], y2_r.at[1 - right, b],
                     {"cb": y_right if right else y_left})

    def wz_copy(dest, source):
        return rcopy(ws_ref.at[dest], wfull.at[source, dp], wz_s.at[dest], wz_r.at[source],
                     {"ra": dest})

    def wx_copy(b, right, share, src=None):
        ref = wfull.at[b, share]
        return rcopy(ref if src is None else src, ref, wx_s.at[1 - right, b], wx_r.at[1 - right, b],
                     {"dp": x_right if right else x_left})

    def wo_copy(b, right, share):
        ref = wfull.at[b, share]
        return rcopy(ref, ref, wo_s.at[b], wo_r.at[b], {"dp": x_right if right else x_left})

    def wp_copy(b, k, share, src=None):
        ref = wfull.at[b, share]
        return rcopy(ref if src is None else src, ref, wp_s.at[k, b], wp_r.at[k, b], {"dp": partner})

    def sq_copy(dest, source):
        return rcopy(sq_ref, sq_all.at[source], sq_s.at[dest], sq_r.at[source], {"ra": dest})

    def w_issue(d):
        @pl.when(d <= half)
        def _():
            wz_copy(zmod(z + d), z).start()
            sq_copy(zmod(z + d), z).start()

        @pl.when(d < half)
        def _():
            wz_copy(zmod(z - d), z).start()
            sq_copy(zmod(z - d), z).start()

    def both(d, fn):
        fn(zmod(z - d))

        @pl.when((d > 0) & (d < half))
        def _():
            fn(zmod(z + d))

    def w_arrive(b):
        wz_copy(b, b).wait_recv()
        wp_copy(b, 0, dp).start()
        wx_copy(b, 1, dp).start()
        wx_copy(b, 0, dp).start()

    def w_side(b):
        wx_copy(b, 1, x_left).wait_recv()
        wx_copy(b, 0, x_right).wait_recv()
        wp_copy(b, 1, x_left).start()
        wp_copy(b, 2, x_right).start()

        @pl.when(lax.rem(b, 2) == 0)
        def _():
            wo_copy(b, 1, x_left).start()

        @pl.when(lax.rem(b, 2) == 1)
        def _():
            wo_copy(b, 0, x_right).start()

    def w_far(b):
        wo_copy(b, 1, x_far).wait_recv()
        wp_copy(b, 3, x_far).start()

    def w_last(b):
        wp_copy(b, 0, partner).wait_recv()
        wp_copy(b, 1, other(x_left)).wait_recv()
        wp_copy(b, 2, other(x_right)).wait_recv()
        wp_copy(b, 3, other(x_far)).wait_recv()

    def x_first(b):
        y1_copy(b, 1, y).start()
        y1_copy(b, 0, y).start()

    def x_second(b):
        y1_copy(b, 1, y_left).wait_recv()
        y2_copy(b, 1, y_left).start()
        y1_copy(b, 0, y_right).wait_recv()
        y2_copy(b, 0, y_right).start()

    def x_third(b):
        y2_copy(b, 1, y_far).wait_recv()
        y2_copy(b, 0, y_far).wait_recv()

    xz_copy(z, 1, xw_ref.at[q_rows(y)]).start()
    xz_copy(z, 0, xw_ref.at[q_rows(y)]).start()
    sq_ref[...] = jnp.sum(jnp.transpose(values * values, (1, 0)), axis=0, keepdims=True)
    loads[0].wait()
    loads[1].wait()
    tail = jnp.zeros((rows, lanes - 2 * units), BF16)
    for j in range(nz):
        cut = slice(j * units, (j + 1) * units)
        ws_ref[j] = jnp.concatenate([wrows[0, :, cut], wrows[1, :, cut], tail], axis=1)
    xfull[z] = xw_ref[...]
    wfull[z, dp] = ws_ref[z]
    sq_all[z] = sq_ref[...]
    w_issue(1)
    wp_copy(z, 0, dp, ws_ref.at[z]).start()
    wx_copy(z, 1, dp, ws_ref.at[z]).start()
    wx_copy(z, 0, dp, ws_ref.at[z]).start()

    acc[...] = jnp.zeros_like(acc)
    loads[6].wait()
    loads[7].wait()
    taps_in[0:3] = taps_g[...]
    taps_in[3:6] = taps_u[...]
    taps_in[6:8] = jnp.zeros((2, taps_in.shape[1]), F32)
    taps_ref[...] = jnp.transpose(taps_in[...], (1, 0))

    def product(b):
        w_last(b)
        w = wfull[b].reshape(kb, lanes)
        acc[...] += jnp.dot(xfull[b], w, preferred_element_type=F32)

    def with_first(d, fn):
        @pl.when((d >= 2) & (d <= half))
        def _():
            @pl.when(d == 2)
            def _():
                both(1, fn)

            both(d, fn)

    @pl.loop(1, half + 4)
    def _(s):
        @pl.when(s <= half)
        def _():
            br = zmod(z - s)
            xz_copy(br, 1).wait_recv()

            @pl.when(s < half)
            def _():
                xz_copy(br, 1).start()

            x_first(br)

            @pl.when(s < half)
            def _():
                bl = zmod(z + s)
                xz_copy(bl, 0).wait_recv()

                @pl.when(s < half - 1)
                def _():
                    xz_copy(bl, 0).start()

                x_first(bl)

        heard(2 * s)

        @pl.when(s <= 2)
        def _():
            w_issue(s + 1)

        @pl.when(s >= 2)
        def _():
            w_issue(s + 2)

        @pl.when((s >= 2) & (s <= half + 1))
        def _():
            both(s - 1, x_second)

        heard(2 * s + 1)

        with_first(s, w_arrive)

        @pl.when(s == 1)
        def _():
            w_side(z)

        with_first(s - 1, w_side)

        @pl.when(s == 2)
        def _():
            w_far(z)

        with_first(s - 2, w_far)

        @pl.when((s >= 3) & (s <= half + 2))
        def _():
            both(s - 2, x_third)

        @pl.when(s == 3)
        def _():
            product(z)

        with_first(s - 3, product)

    @pl.loop(1, nz)
    def _(d):
        src = zmod(z + d)
        sq_copy(src, src).wait_recv()

    scale = lax.rsqrt(jnp.sum(sq_all[...], axis=0) / dim_full + EPS)
    lin[...] = jnp.transpose(acc[...], (1, 0))
    step_rows = -(-units // 64) * 16
    cuts = [(r, min(step_rows, units - r)) for r in range(0, units, step_rows)]
    subs = len(cuts)

    def hz_copy(b, c, right):
        ref = hfull.at[b, pl.ds(*cuts[c])]
        return rcopy(ref, ref, hz_s.at[1 - right, b, c], hz_r.at[b, c],
                     {"ra": z_right if right else z_left})

    def conv(field, taps, base):
        lane = lax.broadcasted_iota(jnp.int32, field.shape, 1)
        before = jnp.where(lane == 0, 0.0, pltpu.roll(field, 1, 1))
        after = jnp.where(lane == tokens - 1, 0.0, pltpu.roll(field, tokens - 1, 1))
        return (
            taps[:, base : base + 1] * before
            + taps[:, base + 1 : base + 2] * field
            + taps[:, base + 2 : base + 3] * after
        )

    for c, (r, count) in enumerate(cuts):
        taps = taps_ref[pl.ds(pl.multiple_of(z * units + r, 16), count), :]
        gate = conv(lin[r : r + count] * scale, taps, 0)
        up = conv(lin[units + r : units + r + count] * scale, taps, 3)
        hfull[z, r : r + count] = (jax.nn.gelu(gate, approximate=True) * up).astype(BF16)
        hz_copy(z, c, 1).start()
        hz_copy(z, c, 0).start()

    def drain_first(b):
        wx_copy(b, 1, dp).wait_send()
        wx_copy(b, 0, dp).wait_send()
        wo_copy(b, 1, x_left).wait_send()
        for k in range(4):
            wp_copy(b, k, dp).wait_send()

        @pl.when(b != z)
        def _():
            y1_copy(b, 1, y).wait_send()
            y1_copy(b, 0, y).wait_send()
            y2_copy(b, 1, y_left).wait_send()
            y2_copy(b, 0, y_right).wait_send()
            wz_copy(b, z).wait_send()
            sq_copy(b, z).wait_send()

    def down(b):
        w = wd_ref[pl.ds(pl.multiple_of(b * units, units), units), :]
        return lax.dot_general(w, hfull[b], (((0,), (0,)), ((), ())), preferred_element_type=F32)

    loads[2].wait()
    loads[5].wait()
    part[...] = down(z)

    @pl.loop(1, half)
    def _(s):
        br, bl = zmod(z - s), zmod(z + s)
        for c in range(subs):
            hz_copy(br, c, 1).wait_recv()
            if c < subs // 2:
                hz_copy(br, c, 1).start()
            else:
                @pl.when(s < half - 1)
                def _():
                    hz_copy(br, c, 1).start()
            hz_copy(bl, c, 0).wait_recv()
            if c >= subs // 2:
                hz_copy(bl, c, 0).start()
            else:
                @pl.when(s < half - 1)
                def _():
                    hz_copy(bl, c, 0).start()
        part[...] += down(br)
        part[...] += down(bl)
        drain_first(br)
        drain_first(bl)

    far = zmod(z + half)
    for c in range(subs):
        hz_copy(far, c, 1 if c < subs // 2 else 0).wait_recv()
    part[...] += down(far)

    def ps_copy(k, dest):
        return rcopy(psend.at[k], precv.at[k], ps_s.at[k], ps_r.at[k], {"cb": dest})

    def quarter_cols(q):
        return pl.ds(pl.multiple_of(q * quarter, quarter), quarter)

    for k, dest in enumerate((y_far, y_right, y_left)):
        psend[k] = part[:, quarter_cols(dest)].astype(BF16)
        ps_copy(k, dest).start()

    for c in range(subs):
        first = c < subs // 2

        @pl.loop(0, half)
        def _(t):
            @pl.when(t < (half if first else half - 1))
            def _():
                hz_copy(zmod(z - t), c, 1).wait_send()

            @pl.when(t < (half - 1 if first else half))
            def _():
                hz_copy(zmod(z + t), c, 0).wait_send()

    @pl.loop(0, half)
    def _(t):
        xz_copy(zmod(z - t), 1).wait_send()

        @pl.when(t < half - 1)
        def _():
            xz_copy(zmod(z + t), 0).wait_send()

    drain_first(z)
    drain_first(far)
    share = part[:, quarter_cols(y)]
    for k, dest in enumerate((y_far, y_right, y_left)):
        ps_copy(k, dest).wait_recv()
        share = share + precv[k].astype(F32)

    def pq_copy(dest, source):
        return rcopy(psq_own, psq_all.at[source], pq_s.at[dest], pq_r.at[source], {"ra": dest})

    own_sq = jnp.sum(share * share, axis=0, keepdims=True)
    psq_own[...] = own_sq
    psq_all[z] = own_sq

    @pl.loop(1, nz)
    def _(d):
        pq_copy(zmod(z + d), z).start()

    branch = jnp.transpose(share, (1, 0)) * gain_ref[...]
    bshare[...] = branch.astype(BF16)

    def mo_copy(k, dest):
        return rcopy(bshare, bfull.at[k], mo_s.at[k], mo_r.at[k], {"cb": dest})

    def po_copy(k, dest):
        return rcopy(post_own, post_all.at[k], po_s.at[k], po_r.at[k], {"cb": dest})

    peers = (y_far, y_right, y_left)
    for k, dest in enumerate(peers):
        mo_copy(k, dest).start()

    @pl.loop(1, nz)
    def _(d):
        src = zmod(z + d)
        pq_copy(src, src).wait_recv()

    post = lax.rsqrt(jnp.sum(psq_all[...], axis=0) / dim_full + EPS)
    post_own[...] = post
    for k, dest in enumerate(peers):
        po_copy(k, dest).start()

    def finish(q, value, scale_row):
        col = jnp.transpose(jnp.broadcast_to(scale_row, (quarter, quarter)), (1, 0))[:, :1]
        base = RESIDUAL * tok_ref[q_rows(q), :].astype(F32)
        out_ref[q_rows(q), :] = (base + value * col).astype(BF16)

    for k, dest in enumerate(peers):
        ps_copy(k, dest).wait_send()

    @pl.loop(1, nz)
    def _(d):
        pq_copy(zmod(z + d), z).wait_send()

    finish(y, branch, post)
    for k, source in enumerate((y_far, y_left, y_right)):
        mo_copy(k, source).wait_recv()
        po_copy(k, source).wait_recv()
        finish(source, bfull[k].astype(F32), post_all[k])

    for k, dest in enumerate(peers):
        mo_copy(k, dest).wait_send()
        po_copy(k, dest).wait_send()


def local(tokens, pre_gain, w_gate, w_up, conv_gate, conv_up, w_down, post_gain):
    nz = lax.axis_size("ra")
    _, positions, kb = tokens.shape
    ff = w_gate.shape[1]
    units = ff // nz
    lanes = -(-2 * units // 128) * 128
    rows = kb // 8
    quarter = positions // 4
    subs = -(-units // (-(-units // 64) * 16))
    dim_full = kb * nz

    dma = pltpu.SemaphoreType.DMA
    vmem = pltpu.VMEM
    scratch = [
        vmem((positions, kb), BF16),
        vmem((1, kb), F32),
        vmem((1, kb), F32),
        vmem((positions, kb), BF16),
        vmem((1, positions), F32),
        vmem((nz, rows, lanes), BF16),
        vmem((2, rows, ff), BF16),
        vmem((ff, kb), BF16),
        vmem((3, ff), F32),
        vmem((3, ff), F32),
        vmem((8, ff), F32),
        vmem((ff, 8), F32),
        vmem((nz, positions, kb), BF16),
        vmem((nz, 8, rows, lanes), BF16),
        vmem((nz, units, positions), BF16),
        vmem((positions, lanes), F32),
        vmem((lanes, positions), F32),
        vmem((kb, positions), F32),
        vmem((3, kb, quarter), BF16),
        vmem((3, kb, quarter), BF16),
        vmem((nz, 1, positions), F32),
        vmem((1, quarter), F32),
        vmem((nz, 1, quarter), F32),
        vmem((quarter, kb), BF16),
        vmem((3, quarter, kb), BF16),
        vmem((1, quarter), F32),
        vmem((3, 1, quarter), F32),
        dma((8,)),
        dma((2, nz)), dma((nz,)),
        dma((2, nz)), dma((2, nz)), dma((2, nz)), dma((2, nz)),
        dma((nz,)), dma((nz,)), dma((2, nz)), dma((2, nz)), dma((nz,)), dma((nz,)),
        dma((4, nz)), dma((4, nz)),
        dma((nz,)), dma((nz,)), dma((2, nz, subs)), dma((nz, subs)),
        dma((3,)), dma((3,)), dma((nz,)), dma((nz,)), dma((3,)), dma((3,)), dma((3,)), dma((3,)),
        pltpu.SemaphoreType.REGULAR, pltpu.SemaphoreType.REGULAR,
    ]

    here = pl.BlockSpec(memory_space=pltpu.VMEM)
    away = pl.BlockSpec(memory_space=pl.ANY)
    out = pl.pallas_call(
        functools.partial(_kernel, dim_full, nz),
        out_shape=jax.ShapeDtypeStruct((positions, kb), BF16),
        in_specs=[away] * 8,
        out_specs=pl.BlockSpec(memory_space=pltpu.VMEM),
        scratch_shapes=scratch,
        name="ffn",
        compiler_params=pltpu.CompilerParams(
            collective_id=0, has_side_effects=True, vmem_limit_bytes=67043328
        ),
    )(tokens[0], pre_gain[None, :], w_gate, w_up, conv_gate, conv_up, w_down, post_gain[None, :])
    return out[None]


def solution(mesh):
    in_specs = (
        P("dp", None, "ra"),
        P("ra"),
        P("ra", "cb"),
        P("ra", "cb"),
        P(None, "cb"),
        P(None, "cb"),
        P("cb", "ra"),
        P("ra"),
    )
    out_specs = P("dp", None, "ra")
    return jax.shard_map(local, mesh=mesh, in_specs=in_specs, out_specs=out_specs, check_vma=False)
```

```python
import functools
import jax
import jax.numpy as jnp
from jax import lax
from jax.experimental import pallas as pl
from jax.experimental.pallas import tpu as pltpu
from jax.sharding import PartitionSpec as P

EPS = 1e-06
RESIDUAL = 0.125
MESH = pl.DeviceIdType.MESH
BF16 = jnp.bfloat16
F32 = jnp.float32


def _kernel(
    dim_full,
    nz,
    tok_in, pre_in, wg_ref, wu_ref, cg_ref, cu_ref, wd_hbm, gain_in,
    out_ref,
    tok_ref, pre_ref, gain_ref, xw_ref, sq_ref, ws_ref, wrows, wd_ref, taps_g, taps_u, taps_in, taps_ref,
    xfull, wfull, hfull, acc, lin, part, psend, precv, sq_all, psq_own, psq_all,
    bshare, bfull, post_own, post_all, in_sem,
    xz_s, xz_r, y1_s, y1_r, y2_s, y2_r, wz_s, wz_r, wx_s, wx_r, wo_s, wo_r, wp_s, wp_r,
    sq_s, sq_r, hz_s, hz_r, ps_s, ps_r, pq_s, pq_r, mo_s, mo_r, po_s, po_r, in_right, in_left,
):
    half = nz // 2
    z = lax.axis_index("ra")
    y = lax.axis_index("cb")
    dp = lax.axis_index("dp")
    tokens, kb = xw_ref.shape
    quarter = tokens // 4
    qhalf = quarter // 2
    units = hfull.shape[1]
    rows = wrows.shape[1]
    lanes = acc.shape[1]

    def zmod(v):
        return lax.rem(v + 2 * nz, nz)

    z_right, z_left = zmod(z + 1), zmod(z - 1)
    y_right, y_left, y_far = lax.rem(y + 1, 4), lax.rem(y + 3, 4), lax.rem(y + 2, 4)
    x_right, x_left = lax.rem(dp + 2, 8), lax.rem(dp + 6, 8)
    x_far = lax.rem(dp + 4, 8)
    partner = dp + 1 - 2 * lax.rem(dp, 2)

    def other(v):
        return v + 1 - 2 * lax.rem(v, 2)

    def rcopy(src, dst, ssem, rsem, dev):
        return pltpu.make_async_remote_copy(
            src_ref=src, dst_ref=dst, send_sem=ssem, recv_sem=rsem,
            device_id=dev, device_id_type=MESH,
        )

    bar = pltpu.get_barrier_semaphore()

    for t in (z_right, z_left):
        pl.semaphore_signal(bar, inc=1, device_id={"ra": t}, device_id_type=MESH)
    for t in (y_right, y_left, y_far):
        pl.semaphore_signal(bar, inc=1, device_id={"cb": t}, device_id_type=MESH)
    for t in (x_right, x_left, partner):
        pl.semaphore_signal(bar, inc=1, device_id={"dp": t}, device_id_type=MESH)

    own = pl.ds(pl.multiple_of(dp * rows, rows), rows)
    loads = [
        pltpu.make_async_copy(wg_ref.at[own], wrows.at[0], in_sem.at[0]),
        pltpu.make_async_copy(wu_ref.at[own], wrows.at[1], in_sem.at[1]),
        pltpu.make_async_copy(wd_hbm, wd_ref, in_sem.at[2]),
        pltpu.make_async_copy(tok_in, tok_ref, in_sem.at[3]),
        pltpu.make_async_copy(pre_in, pre_ref, in_sem.at[4]),
        pltpu.make_async_copy(gain_in, gain_ref, in_sem.at[5]),
        pltpu.make_async_copy(cg_ref, taps_g, in_sem.at[6]),
        pltpu.make_async_copy(cu_ref, taps_u, in_sem.at[7]),
    ]
    for k in (3, 4, 0, 1, 5, 6, 7, 2):
        loads[k].start()
    loads[3].wait()
    loads[4].wait()
    values = tok_ref[...].astype(F32)
    xw_ref[...] = (values * pre_ref[...]).astype(BF16)
    pl.semaphore_wait(bar, 8)

    def relay(k):
        @pl.when(k <= half)
        def _():
            pl.semaphore_signal(in_right, inc=1, device_id={"ra": z_right}, device_id_type=MESH)

        @pl.when(k < half)
        def _():
            pl.semaphore_signal(in_left, inc=1, device_id={"ra": z_left}, device_id_type=MESH)

    def heard(k):
        @pl.when(k <= half)
        def _():
            pl.semaphore_wait(in_right, 1)

        @pl.when(k < half)
        def _():
            pl.semaphore_wait(in_left, 1)

        relay(k + 1)

    relay(2)

    def q_rows(q):
        return pl.ds(pl.multiple_of(q * quarter, quarter), quarter)

    def qh_rows(q, i):
        return pl.ds(pl.multiple_of(q * quarter + i * qhalf, qhalf), qhalf)

    def xz_copy(b, i, right, src=None):
        ref = (xfull.at[b] if src is None else src).at[qh_rows(y, i)]
        return rcopy(ref, xfull.at[b, qh_rows(y, i)], xz_s.at[1 - right, b, i], xz_r.at[b, i],
                     {"ra": z_right if right else z_left})

    def y1_copy(b, right, q):
        ref = xfull.at[b, q_rows(q)]
        return rcopy(ref, ref, y1_s.at[1 - right, b], y1_r.at[1 - right, b],
                     {"cb": y_right if right else y_left})

    def y2_copy(b, right, q):
        ref = xfull.at[b, qh_rows(q, 1 - right)]
        return rcopy(ref, ref, y2_s.at[1 - right, b], y2_r.at[1 - right, b],
                     {"cb": y_right if right else y_left})

    def wz_copy(dest, source):
        return rcopy(ws_ref.at[dest], wfull.at[source, dp], wz_s.at[dest], wz_r.at[source],
                     {"ra": dest})

    def wx_copy(b, right, share, src=None):
        ref = wfull.at[b, share]
        return rcopy(ref if src is None else src, ref, wx_s.at[1 - right, b], wx_r.at[1 - right, b],
                     {"dp": x_right if right else x_left})

    def wo_copy(b, right, share):
        ref = wfull.at[b, share]
        return rcopy(ref, ref, wo_s.at[b], wo_r.at[b], {"dp": x_right if right else x_left})

    def wp_copy(b, k, share, src=None):
        ref = wfull.at[b, share]
        return rcopy(ref if src is None else src, ref, wp_s.at[k, b], wp_r.at[k, b], {"dp": partner})

    def sq_copy(dest, source):
        return rcopy(sq_ref, sq_all.at[source], sq_s.at[dest], sq_r.at[source], {"ra": dest})

    def w_issue(d):
        @pl.when(d <= half)
        def _():
            wz_copy(zmod(z + d), z).start()
            sq_copy(zmod(z + d), z).start()

        @pl.when(d < half)
        def _():
            wz_copy(zmod(z - d), z).start()
            sq_copy(zmod(z - d), z).start()

    def both(d, fn):
        fn(zmod(z - d))

        @pl.when((d > 0) & (d < half))
        def _():
            fn(zmod(z + d))

    def w_arrive(b):
        wz_copy(b, b).wait_recv()
        wp_copy(b, 0, dp).start()
        wx_copy(b, 1, dp).start()
        wx_copy(b, 0, dp).start()

    def w_side(b):
        wx_copy(b, 1, x_left).wait_recv()
        wx_copy(b, 0, x_right).wait_recv()
        wp_copy(b, 1, x_left).start()
        wp_copy(b, 2, x_right).start()

        @pl.when(lax.rem(b, 2) == 0)
        def _():
            wo_copy(b, 1, x_left).start()

        @pl.when(lax.rem(b, 2) == 1)
        def _():
            wo_copy(b, 0, x_right).start()

    def w_far(b):
        wo_copy(b, 1, x_far).wait_recv()
        wp_copy(b, 3, x_far).start()

    def w_last(b):
        wp_copy(b, 0, partner).wait_recv()
        wp_copy(b, 1, other(x_left)).wait_recv()
        wp_copy(b, 2, other(x_right)).wait_recv()
        wp_copy(b, 3, other(x_far)).wait_recv()

    def x_first(b):
        y1_copy(b, 1, y).start()
        y1_copy(b, 0, y).start()

    def x_second(b):
        y1_copy(b, 1, y_left).wait_recv()
        y2_copy(b, 1, y_left).start()
        y1_copy(b, 0, y_right).wait_recv()
        y2_copy(b, 0, y_right).start()

    def x_third(b):
        y2_copy(b, 1, y_far).wait_recv()
        y2_copy(b, 0, y_far).wait_recv()

    for i in range(2):
        xz_copy(z, i, 1, xw_ref).start()
        xz_copy(z, i, 0, xw_ref).start()
    sq_ref[...] = jnp.sum(jnp.transpose(values * values, (1, 0)), axis=0, keepdims=True)
    loads[0].wait()
    loads[1].wait()
    tail = jnp.zeros((rows, lanes - 2 * units), BF16)
    for j in range(nz):
        cut = slice(j * units, (j + 1) * units)
        ws_ref[j] = jnp.concatenate([wrows[0, :, cut], wrows[1, :, cut], tail], axis=1)
    xfull[z] = xw_ref[...]
    wfull[z, dp] = ws_ref[z]
    sq_all[z] = sq_ref[...]
    w_issue(1)
    wp_copy(z, 0, dp, ws_ref.at[z]).start()
    wx_copy(z, 1, dp, ws_ref.at[z]).start()
    wx_copy(z, 0, dp, ws_ref.at[z]).start()

    acc[...] = jnp.zeros_like(acc)
    loads[6].wait()
    loads[7].wait()
    taps_in[0:3] = taps_g[...]
    taps_in[3:6] = taps_u[...]
    taps_in[6:8] = jnp.zeros((2, taps_in.shape[1]), F32)
    taps_ref[...] = jnp.transpose(taps_in[...], (1, 0))

    def product(b):
        w_last(b)
        w = wfull[b].reshape(kb, lanes)
        acc[...] += jnp.dot(xfull[b], w, preferred_element_type=F32)

    def with_first(d, fn):
        @pl.when((d >= 2) & (d <= half))
        def _():
            @pl.when(d == 2)
            def _():
                both(1, fn)

            both(d, fn)

    @pl.loop(1, half + 4)
    def _(s):
        @pl.when(s <= half)
        def _():
            br = zmod(z - s)
            for i in range(2):
                xz_copy(br, i, 1).wait_recv()

                @pl.when(s < half)
                def _():
                    xz_copy(br, i, 1).start()

            x_first(br)

            @pl.when(s < half)
            def _():
                bl = zmod(z + s)
                for i in range(2):
                    xz_copy(bl, i, 0).wait_recv()

                    @pl.when(s < half - 1)
                    def _():
                        xz_copy(bl, i, 0).start()

                x_first(bl)

        heard(2 * s)

        @pl.when(s <= 2)
        def _():
            w_issue(s + 1)

        @pl.when(s >= 2)
        def _():
            w_issue(s + 2)

        @pl.when((s >= 2) & (s <= half + 1))
        def _():
            both(s - 1, x_second)

        heard(2 * s + 1)

        with_first(s, w_arrive)

        @pl.when(s == 1)
        def _():
            w_side(z)

        with_first(s - 1, w_side)

        @pl.when(s == 2)
        def _():
            w_far(z)

        with_first(s - 2, w_far)

        @pl.when((s >= 3) & (s <= half + 2))
        def _():
            both(s - 2, x_third)

        @pl.when(s == 3)
        def _():
            product(z)

        with_first(s - 3, product)

    @pl.loop(1, nz)
    def _(d):
        src = zmod(z + d)
        sq_copy(src, src).wait_recv()

    scale = lax.rsqrt(jnp.sum(sq_all[...], axis=0) / dim_full + EPS)
    lin[...] = jnp.transpose(acc[...], (1, 0))
    step_rows = -(-units // 64) * 16
    cuts = [(r, min(step_rows, units - r)) for r in range(0, units, step_rows)]
    subs = len(cuts)

    def hz_copy(b, c, right):
        ref = hfull.at[b, pl.ds(*cuts[c])]
        return rcopy(ref, ref, hz_s.at[1 - right, b, c], hz_r.at[b, c],
                     {"ra": z_right if right else z_left})

    def conv(field, taps, base):
        lane = lax.broadcasted_iota(jnp.int32, field.shape, 1)
        before = jnp.where(lane == 0, 0.0, pltpu.roll(field, 1, 1))
        after = jnp.where(lane == tokens - 1, 0.0, pltpu.roll(field, tokens - 1, 1))
        return (
            taps[:, base : base + 1] * before
            + taps[:, base + 1 : base + 2] * field
            + taps[:, base + 2 : base + 3] * after
        )

    for c, (r, count) in enumerate(cuts):
        taps = taps_ref[pl.ds(pl.multiple_of(z * units + r, 16), count), :]
        gate = conv(lin[r : r + count] * scale, taps, 0)
        up = conv(lin[units + r : units + r + count] * scale, taps, 3)
        hfull[z, r : r + count] = (jax.nn.gelu(gate, approximate=True) * up).astype(BF16)
        hz_copy(z, c, 1).start()
        hz_copy(z, c, 0).start()

    def drain_first(b):
        wx_copy(b, 1, dp).wait_send()
        wx_copy(b, 0, dp).wait_send()
        wo_copy(b, 1, x_left).wait_send()
        for k in range(4):
            wp_copy(b, k, dp).wait_send()

        @pl.when(b != z)
        def _():
            y1_copy(b, 1, y).wait_send()
            y1_copy(b, 0, y).wait_send()
            y2_copy(b, 1, y_left).wait_send()
            y2_copy(b, 0, y_right).wait_send()
            wz_copy(b, z).wait_send()
            sq_copy(b, z).wait_send()

    def down(b):
        w = wd_ref[pl.ds(pl.multiple_of(b * units, units), units), :]
        return lax.dot_general(w, hfull[b], (((0,), (0,)), ((), ())), preferred_element_type=F32)

    loads[2].wait()
    loads[5].wait()
    part[...] = down(z)

    @pl.loop(1, half)
    def _(s):
        br, bl = zmod(z - s), zmod(z + s)
        for c in range(subs):
            hz_copy(br, c, 1).wait_recv()
            if c < subs // 2:
                hz_copy(br, c, 1).start()
            else:
                @pl.when(s < half - 1)
                def _():
                    hz_copy(br, c, 1).start()
            hz_copy(bl, c, 0).wait_recv()
            if c >= subs // 2:
                hz_copy(bl, c, 0).start()
            else:
                @pl.when(s < half - 1)
                def _():
                    hz_copy(bl, c, 0).start()
        part[...] += down(br)
        part[...] += down(bl)
        drain_first(br)
        drain_first(bl)

    far = zmod(z + half)
    for c in range(subs):
        hz_copy(far, c, 1 if c < subs // 2 else 0).wait_recv()
    part[...] += down(far)

    def ps_copy(k, dest):
        return rcopy(psend.at[k], precv.at[k], ps_s.at[k], ps_r.at[k], {"cb": dest})

    def quarter_cols(q):
        return pl.ds(pl.multiple_of(q * quarter, quarter), quarter)

    for k, dest in enumerate((y_far, y_right, y_left)):
        psend[k] = part[:, quarter_cols(dest)].astype(BF16)
        ps_copy(k, dest).start()

    for c in range(subs):
        first = c < subs // 2

        @pl.loop(0, half)
        def _(t):
            @pl.when(t < (half if first else half - 1))
            def _():
                hz_copy(zmod(z - t), c, 1).wait_send()

            @pl.when(t < (half - 1 if first else half))
            def _():
                hz_copy(zmod(z + t), c, 0).wait_send()

    @pl.loop(0, half)
    def _(t):
        for i in range(2):
            xz_copy(zmod(z - t), i, 1).wait_send()

        @pl.when(t < half - 1)
        def _():
            for i in range(2):
                xz_copy(zmod(z + t), i, 0).wait_send()

    drain_first(z)
    drain_first(far)
    share = part[:, quarter_cols(y)]
    for k, dest in enumerate((y_far, y_right, y_left)):
        ps_copy(k, dest).wait_recv()
        share = share + precv[k].astype(F32)

    def pq_copy(dest, source):
        return rcopy(psq_own, psq_all.at[source], pq_s.at[dest], pq_r.at[source], {"ra": dest})

    own_sq = jnp.sum(share * share, axis=0, keepdims=True)
    psq_own[...] = own_sq
    psq_all[z] = own_sq

    @pl.loop(1, nz)
    def _(d):
        pq_copy(zmod(z + d), z).start()

    branch = jnp.transpose(share, (1, 0)) * gain_ref[...]
    bshare[...] = branch.astype(BF16)

    def mo_copy(k, dest):
        return rcopy(bshare, bfull.at[k], mo_s.at[k], mo_r.at[k], {"cb": dest})

    def po_copy(k, dest):
        return rcopy(post_own, post_all.at[k], po_s.at[k], po_r.at[k], {"cb": dest})

    peers = (y_far, y_right, y_left)
    for k, dest in enumerate(peers):
        mo_copy(k, dest).start()

    @pl.loop(1, nz)
    def _(d):
        src = zmod(z + d)
        pq_copy(src, src).wait_recv()

    post = lax.rsqrt(jnp.sum(psq_all[...], axis=0) / dim_full + EPS)
    post_own[...] = post
    for k, dest in enumerate(peers):
        po_copy(k, dest).start()

    def finish(q, value, scale_row):
        col = jnp.transpose(jnp.broadcast_to(scale_row, (quarter, quarter)), (1, 0))[:, :1]
        base = RESIDUAL * tok_ref[q_rows(q), :].astype(F32)
        out_ref[q_rows(q), :] = (base + value * col).astype(BF16)

    for k, dest in enumerate(peers):
        ps_copy(k, dest).wait_send()

    @pl.loop(1, nz)
    def _(d):
        pq_copy(zmod(z + d), z).wait_send()

    finish(y, branch, post)
    for k, source in enumerate((y_far, y_left, y_right)):
        mo_copy(k, source).wait_recv()
        po_copy(k, source).wait_recv()
        finish(source, bfull[k].astype(F32), post_all[k])

    for k, dest in enumerate(peers):
        mo_copy(k, dest).wait_send()
        po_copy(k, dest).wait_send()


def local(tokens, pre_gain, w_gate, w_up, conv_gate, conv_up, w_down, post_gain):
    nz = lax.axis_size("ra")
    _, positions, kb = tokens.shape
    ff = w_gate.shape[1]
    units = ff // nz
    lanes = -(-2 * units // 128) * 128
    rows = kb // 8
    quarter = positions // 4
    subs = -(-units // (-(-units // 64) * 16))
    dim_full = kb * nz

    dma = pltpu.SemaphoreType.DMA
    vmem = pltpu.VMEM
    scratch = [
        vmem((positions, kb), BF16),
        vmem((1, kb), F32),
        vmem((1, kb), F32),
        vmem((positions, kb), BF16),
        vmem((1, positions), F32),
        vmem((nz, rows, lanes), BF16),
        vmem((2, rows, ff), BF16),
        vmem((ff, kb), BF16),
        vmem((3, ff), F32),
        vmem((3, ff), F32),
        vmem((8, ff), F32),
        vmem((ff, 8), F32),
        vmem((nz, positions, kb), BF16),
        vmem((nz, 8, rows, lanes), BF16),
        vmem((nz, units, positions), BF16),
        vmem((positions, lanes), F32),
        vmem((lanes, positions), F32),
        vmem((kb, positions), F32),
        vmem((3, kb, quarter), BF16),
        vmem((3, kb, quarter), BF16),
        vmem((nz, 1, positions), F32),
        vmem((1, quarter), F32),
        vmem((nz, 1, quarter), F32),
        vmem((quarter, kb), BF16),
        vmem((3, quarter, kb), BF16),
        vmem((1, quarter), F32),
        vmem((3, 1, quarter), F32),
        dma((8,)),
        dma((2, nz, 2)), dma((nz, 2)),
        dma((2, nz)), dma((2, nz)), dma((2, nz)), dma((2, nz)),
        dma((nz,)), dma((nz,)), dma((2, nz)), dma((2, nz)), dma((nz,)), dma((nz,)),
        dma((4, nz)), dma((4, nz)),
        dma((nz,)), dma((nz,)), dma((2, nz, subs)), dma((nz, subs)),
        dma((3,)), dma((3,)), dma((nz,)), dma((nz,)), dma((3,)), dma((3,)), dma((3,)), dma((3,)),
        pltpu.SemaphoreType.REGULAR, pltpu.SemaphoreType.REGULAR,
    ]

    here = pl.BlockSpec(memory_space=pltpu.VMEM)
    away = pl.BlockSpec(memory_space=pl.ANY)
    out = pl.pallas_call(
        functools.partial(_kernel, dim_full, nz),
        out_shape=jax.ShapeDtypeStruct((positions, kb), BF16),
        in_specs=[away] * 8,
        out_specs=pl.BlockSpec(memory_space=pltpu.VMEM),
        scratch_shapes=scratch,
        name="ffn",
        compiler_params=pltpu.CompilerParams(
            collective_id=0, has_side_effects=True, vmem_limit_bytes=67043328
        ),
    )(tokens[0], pre_gain[None, :], w_gate, w_up, conv_gate, conv_up, w_down, post_gain[None, :])
    return out[None]


def solution(mesh):
    in_specs = (
        P("dp", None, "ra"),
        P("ra"),
        P("ra", "cb"),
        P("ra", "cb"),
        P(None, "cb"),
        P(None, "cb"),
        P("cb", "ra"),
        P("ra"),
    )
    out_specs = P("dp", None, "ra")
    return jax.shard_map(local, mesh=mesh, in_specs=in_specs, out_specs=out_specs, check_vma=False)
```

```python
import functools
import jax
import jax.numpy as jnp
from jax import lax
from jax.experimental import pallas as pl
from jax.experimental.pallas import tpu as pltpu
from jax.sharding import PartitionSpec as P

EPS = 1e-06
RESIDUAL = 0.125
MESH = pl.DeviceIdType.MESH
BF16 = jnp.bfloat16
F32 = jnp.float32


def _kernel(
    dim_full,
    nz,
    tok_in, pre_in, wg_ref, wu_ref, cg_ref, cu_ref, wd_hbm, gain_in,
    out_ref,
    tok_ref, pre_ref, gain_ref, xw_ref, sq_ref, ws_ref, wrows, wd_ref, taps_g, taps_u, taps_in, taps_ref,
    xfull, wfull, hfull, acc, lin, part, psend, precv, sq_all, psq_own, psq_all,
    bshare, bfull, post_own, post_all, in_sem,
    xz_s, xz_r, y1_s, y1_r, y2_s, y2_r, wz_s, wz_r, wx_s, wx_r, wo_s, wo_r, wp_s, wp_r,
    sq_s, sq_r, hz_s, hz_r, ps_s, ps_r, pq_s, pq_r, mo_s, mo_r, po_s, po_r, in_right, in_left,
):
    half = nz // 2
    z = lax.axis_index("ra")
    y = lax.axis_index("cb")
    dp = lax.axis_index("dp")
    tokens, kb = xw_ref.shape
    quarter = tokens // 4
    qhalf = quarter // 2
    units = hfull.shape[1]
    rows = wrows.shape[1]
    lanes = acc.shape[1]

    def zmod(v):
        return lax.rem(v + 2 * nz, nz)

    z_right, z_left = zmod(z + 1), zmod(z - 1)
    y_right, y_left, y_far = lax.rem(y + 1, 4), lax.rem(y + 3, 4), lax.rem(y + 2, 4)
    x_right, x_left = lax.rem(dp + 2, 8), lax.rem(dp + 6, 8)
    x_far = lax.rem(dp + 4, 8)
    partner = dp + 1 - 2 * lax.rem(dp, 2)

    def other(v):
        return v + 1 - 2 * lax.rem(v, 2)

    def rcopy(src, dst, ssem, rsem, dev):
        return pltpu.make_async_remote_copy(
            src_ref=src, dst_ref=dst, send_sem=ssem, recv_sem=rsem,
            device_id=dev, device_id_type=MESH,
        )

    bar = pltpu.get_barrier_semaphore()

    for t in (z_right, z_left):
        pl.semaphore_signal(bar, inc=1, device_id={"ra": t}, device_id_type=MESH)
    for t in (y_right, y_left, y_far):
        pl.semaphore_signal(bar, inc=1, device_id={"cb": t}, device_id_type=MESH)
    for t in (x_right, x_left, partner):
        pl.semaphore_signal(bar, inc=1, device_id={"dp": t}, device_id_type=MESH)

    own = pl.ds(pl.multiple_of(dp * rows, rows), rows)
    loads = [
        pltpu.make_async_copy(wg_ref.at[own], wrows.at[0], in_sem.at[0]),
        pltpu.make_async_copy(wu_ref.at[own], wrows.at[1], in_sem.at[1]),
        pltpu.make_async_copy(wd_hbm, wd_ref, in_sem.at[2]),
        pltpu.make_async_copy(tok_in, tok_ref, in_sem.at[3]),
        pltpu.make_async_copy(pre_in, pre_ref, in_sem.at[4]),
        pltpu.make_async_copy(gain_in, gain_ref, in_sem.at[5]),
        pltpu.make_async_copy(cg_ref, taps_g, in_sem.at[6]),
        pltpu.make_async_copy(cu_ref, taps_u, in_sem.at[7]),
    ]
    for k in (3, 4, 0, 1, 5, 6, 7, 2):
        loads[k].start()
    loads[3].wait()
    loads[4].wait()
    values = tok_ref[...].astype(F32)
    xw_ref[...] = (values * pre_ref[...]).astype(BF16)
    pl.semaphore_wait(bar, 8)

    def relay(k):
        @pl.when(k <= half)
        def _():
            pl.semaphore_signal(in_right, inc=1, device_id={"ra": z_right}, device_id_type=MESH)

        @pl.when(k < half)
        def _():
            pl.semaphore_signal(in_left, inc=1, device_id={"ra": z_left}, device_id_type=MESH)

    def heard(k):
        @pl.when(k <= half)
        def _():
            pl.semaphore_wait(in_right, 1)

        @pl.when(k < half)
        def _():
            pl.semaphore_wait(in_left, 1)

        relay(k + 1)

    relay(2)

    def q_rows(q):
        return pl.ds(pl.multiple_of(q * quarter, quarter), quarter)

    def qh_rows(q, i):
        return pl.ds(pl.multiple_of(q * quarter + i * qhalf, qhalf), qhalf)

    def xz_copy(b, i, right, src=None):
        ref = (xfull.at[b] if src is None else src).at[qh_rows(y, i)]
        return rcopy(ref, xfull.at[b, qh_rows(y, i)], xz_s.at[1 - right, b, i], xz_r.at[b, i],
                     {"ra": z_right if right else z_left})

    def y1_copy(b, right, q):
        ref = xfull.at[b, q_rows(q)]
        return rcopy(ref, ref, y1_s.at[1 - right, b], y1_r.at[1 - right, b],
                     {"cb": y_right if right else y_left})

    def y2_copy(b, right, q):
        ref = xfull.at[b, qh_rows(q, 1 - right)]
        return rcopy(ref, ref, y2_s.at[1 - right, b], y2_r.at[1 - right, b],
                     {"cb": y_right if right else y_left})

    def wz_copy(dest, source):
        return rcopy(ws_ref.at[dest], wfull.at[source, dp], wz_s.at[dest], wz_r.at[source],
                     {"ra": dest})

    def wx_copy(b, right, share, src=None):
        ref = wfull.at[b, share]
        return rcopy(ref if src is None else src, ref, wx_s.at[1 - right, b], wx_r.at[1 - right, b],
                     {"dp": x_right if right else x_left})

    def wo_copy(b, right, share):
        ref = wfull.at[b, share]
        return rcopy(ref, ref, wo_s.at[b], wo_r.at[b], {"dp": x_right if right else x_left})

    def wp_copy(b, k, share, src=None):
        ref = wfull.at[b, share]
        return rcopy(ref if src is None else src, ref, wp_s.at[k, b], wp_r.at[k, b], {"dp": partner})

    def sq_copy(dest, source):
        return rcopy(sq_ref, sq_all.at[source], sq_s.at[dest], sq_r.at[source], {"ra": dest})

    def w_issue(d):
        @pl.when(d <= half)
        def _():
            wz_copy(zmod(z + d), z).start()
            sq_copy(zmod(z + d), z).start()

        @pl.when(d < half)
        def _():
            wz_copy(zmod(z - d), z).start()
            sq_copy(zmod(z - d), z).start()

    def both(d, fn):
        fn(zmod(z - d))

        @pl.when((d > 0) & (d < half))
        def _():
            fn(zmod(z + d))

    def w_arrive(b):
        wz_copy(b, b).wait_recv()
        wp_copy(b, 0, dp).start()
        wx_copy(b, 1, dp).start()
        wx_copy(b, 0, dp).start()

    def w_side(b):
        wx_copy(b, 1, x_left).wait_recv()
        wx_copy(b, 0, x_right).wait_recv()
        wp_copy(b, 1, x_left).start()
        wp_copy(b, 2, x_right).start()

        @pl.when(lax.rem(b, 2) == 0)
        def _():
            wo_copy(b, 1, x_left).start()

        @pl.when(lax.rem(b, 2) == 1)
        def _():
            wo_copy(b, 0, x_right).start()

    def w_far(b):
        wo_copy(b, 1, x_far).wait_recv()
        wp_copy(b, 3, x_far).start()

    def w_last(b):
        wp_copy(b, 0, partner).wait_recv()
        wp_copy(b, 1, other(x_left)).wait_recv()
        wp_copy(b, 2, other(x_right)).wait_recv()
        wp_copy(b, 3, other(x_far)).wait_recv()

    def x_first(b):
        y1_copy(b, 1, y).start()
        y1_copy(b, 0, y).start()

    def x_second(b):
        y1_copy(b, 1, y_left).wait_recv()
        y2_copy(b, 1, y_left).start()
        y1_copy(b, 0, y_right).wait_recv()
        y2_copy(b, 0, y_right).start()

    def x_third(b):
        y2_copy(b, 1, y_far).wait_recv()
        y2_copy(b, 0, y_far).wait_recv()

    for i in range(2):
        xz_copy(z, i, 1, xw_ref).start()
        xz_copy(z, i, 0, xw_ref).start()
    sq_ref[...] = jnp.sum(jnp.transpose(values * values, (1, 0)), axis=0, keepdims=True)
    loads[0].wait()
    loads[1].wait()
    tail = jnp.zeros((rows, lanes - 2 * units), BF16)
    for j in range(nz):
        cut = slice(j * units, (j + 1) * units)
        ws_ref[j] = jnp.concatenate([wrows[0, :, cut], wrows[1, :, cut], tail], axis=1)
    xfull[z] = xw_ref[...]
    wfull[z, dp] = ws_ref[z]
    sq_all[z] = sq_ref[...]
    w_issue(1)
    wp_copy(z, 0, dp, ws_ref.at[z]).start()
    wx_copy(z, 1, dp, ws_ref.at[z]).start()
    wx_copy(z, 0, dp, ws_ref.at[z]).start()

    acc[...] = jnp.zeros_like(acc)
    loads[6].wait()
    loads[7].wait()
    taps_in[0:3] = taps_g[...]
    taps_in[3:6] = taps_u[...]
    taps_in[6:8] = jnp.zeros((2, taps_in.shape[1]), F32)
    taps_ref[...] = jnp.transpose(taps_in[...], (1, 0))

    def product(b):
        w_last(b)
        w = wfull[b].reshape(kb, lanes)
        acc[...] += jnp.dot(xfull[b], w, preferred_element_type=F32)

    def with_first(d, fn):
        @pl.when((d >= 2) & (d <= half))
        def _():
            @pl.when(d == 2)
            def _():
                both(1, fn)

            both(d, fn)

    @pl.loop(1, half + 4)
    def _(s):
        @pl.when(s <= half)
        def _():
            br = zmod(z - s)
            for i in range(2):
                xz_copy(br, i, 1).wait_recv()

                @pl.when(s < half)
                def _():
                    xz_copy(br, i, 1).start()

            x_first(br)

            @pl.when(s < half)
            def _():
                bl = zmod(z + s)
                for i in range(2):
                    xz_copy(bl, i, 0).wait_recv()

                    @pl.when(s < half - 1)
                    def _():
                        xz_copy(bl, i, 0).start()

                x_first(bl)

        heard(2 * s)

        @pl.when(s <= 2)
        def _():
            w_issue(s + 1)

        @pl.when(s >= 2)
        def _():
            w_issue(s + 2)

        @pl.when((s >= 2) & (s <= half + 1))
        def _():
            both(s - 1, x_second)

        heard(2 * s + 1)

        with_first(s, w_arrive)

        @pl.when(s == 1)
        def _():
            w_side(z)

        with_first(s - 1, w_side)

        @pl.when(s == 2)
        def _():
            w_far(z)

        with_first(s - 2, w_far)

        @pl.when((s >= 3) & (s <= half + 2))
        def _():
            both(s - 2, x_third)

        @pl.when(s == 3)
        def _():
            product(z)

        with_first(s - 3, product)

    @pl.loop(1, nz)
    def _(d):
        src = zmod(z + d)
        sq_copy(src, src).wait_recv()

    scale = lax.rsqrt(jnp.sum(sq_all[...], axis=0) / dim_full + EPS)
    lin[...] = jnp.transpose(acc[...], (1, 0))
    step_rows = -(-units // 64) * 16
    cuts = [(r, min(step_rows, units - r)) for r in range(0, units, step_rows)]
    subs = len(cuts)

    def hz_copy(b, c, right):
        ref = hfull.at[b, pl.ds(*cuts[c])]
        return rcopy(ref, ref, hz_s.at[1 - right, b, c], hz_r.at[b, c],
                     {"ra": z_right if right else z_left})

    def conv(field, taps, base):
        lane = lax.broadcasted_iota(jnp.int32, field.shape, 1)
        before = jnp.where(lane == 0, 0.0, pltpu.roll(field, 1, 1))
        after = jnp.where(lane == tokens - 1, 0.0, pltpu.roll(field, tokens - 1, 1))
        return (
            taps[:, base : base + 1] * before
            + taps[:, base + 1 : base + 2] * field
            + taps[:, base + 2 : base + 3] * after
        )

    for c, (r, count) in enumerate(cuts):
        taps = taps_ref[pl.ds(pl.multiple_of(z * units + r, 16), count), :]
        gate = conv(lin[r : r + count] * scale, taps, 0)
        up = conv(lin[units + r : units + r + count] * scale, taps, 3)
        hfull[z, r : r + count] = (jax.nn.gelu(gate, approximate=True) * up).astype(BF16)
        hz_copy(z, c, 1).start()
        hz_copy(z, c, 0).start()

    def drain_first(b):
        wx_copy(b, 1, dp).wait_send()
        wx_copy(b, 0, dp).wait_send()
        wo_copy(b, 1, x_left).wait_send()
        for k in range(4):
            wp_copy(b, k, dp).wait_send()

        @pl.when(b != z)
        def _():
            y1_copy(b, 1, y).wait_send()
            y1_copy(b, 0, y).wait_send()
            y2_copy(b, 1, y_left).wait_send()
            y2_copy(b, 0, y_right).wait_send()
            wz_copy(b, z).wait_send()
            sq_copy(b, z).wait_send()

    def down(b):
        w = wd_ref[pl.ds(pl.multiple_of(b * units, units), units), :]
        return lax.dot_general(w, hfull[b], (((0,), (0,)), ((), ())), preferred_element_type=F32)

    loads[2].wait()
    loads[5].wait()
    part[...] = down(z)

    @pl.loop(1, half)
    def _(s):
        br, bl = zmod(z - s), zmod(z + s)
        for c in range(subs):
            hz_copy(br, c, 1).wait_recv()
            if c < subs // 2:
                hz_copy(br, c, 1).start()
            else:
                @pl.when(s < half - 1)
                def _():
                    hz_copy(br, c, 1).start()
            hz_copy(bl, c, 0).wait_recv()
            if c >= subs // 2:
                hz_copy(bl, c, 0).start()
            else:
                @pl.when(s < half - 1)
                def _():
                    hz_copy(bl, c, 0).start()
        part[...] += down(br)
        part[...] += down(bl)

    far = zmod(z + half)
    for c in range(subs):
        hz_copy(far, c, 1 if c < subs // 2 else 0).wait_recv()
    part[...] += down(far)

    def ps_copy(k, dest):
        return rcopy(psend.at[k], precv.at[k], ps_s.at[k], ps_r.at[k], {"cb": dest})

    def quarter_cols(q):
        return pl.ds(pl.multiple_of(q * quarter, quarter), quarter)

    for k, dest in enumerate((y_far, y_right, y_left)):
        psend[k] = part[:, quarter_cols(dest)].astype(BF16)
        ps_copy(k, dest).start()

    for c in range(subs):
        first = c < subs // 2

        @pl.loop(0, half)
        def _(t):
            @pl.when(t < (half if first else half - 1))
            def _():
                hz_copy(zmod(z - t), c, 1).wait_send()

            @pl.when(t < (half - 1 if first else half))
            def _():
                hz_copy(zmod(z + t), c, 0).wait_send()

    @pl.loop(0, half)
    def _(t):
        for i in range(2):
            xz_copy(zmod(z - t), i, 1).wait_send()

        @pl.when(t < half - 1)
        def _():
            for i in range(2):
                xz_copy(zmod(z + t), i, 0).wait_send()

    share = part[:, quarter_cols(y)]
    for k, dest in enumerate((y_far, y_right, y_left)):
        ps_copy(k, dest).wait_recv()
        share = share + precv[k].astype(F32)

    def pq_copy(dest, source):
        return rcopy(psq_own, psq_all.at[source], pq_s.at[dest], pq_r.at[source], {"ra": dest})

    own_sq = jnp.sum(share * share, axis=0, keepdims=True)
    psq_own[...] = own_sq
    psq_all[z] = own_sq

    @pl.loop(1, nz)
    def _(d):
        pq_copy(zmod(z + d), z).start()

    branch = jnp.transpose(share, (1, 0)) * gain_ref[...]
    bshare[...] = branch.astype(BF16)

    def mo_copy(k, dest):
        return rcopy(bshare, bfull.at[k], mo_s.at[k], mo_r.at[k], {"cb": dest})

    def po_copy(k, dest):
        return rcopy(post_own, post_all.at[k], po_s.at[k], po_r.at[k], {"cb": dest})

    peers = (y_far, y_right, y_left)
    for k, dest in enumerate(peers):
        mo_copy(k, dest).start()

    @pl.loop(0, nz)
    def _(b):
        drain_first(b)

    @pl.loop(1, nz)
    def _(d):
        src = zmod(z + d)
        pq_copy(src, src).wait_recv()

    post = lax.rsqrt(jnp.sum(psq_all[...], axis=0) / dim_full + EPS)
    post_own[...] = post
    for k, dest in enumerate(peers):
        po_copy(k, dest).start()

    def finish(q, value, scale_row):
        col = jnp.transpose(jnp.broadcast_to(scale_row, (quarter, quarter)), (1, 0))[:, :1]
        base = RESIDUAL * tok_ref[q_rows(q), :].astype(F32)
        out_ref[q_rows(q), :] = (base + value * col).astype(BF16)

    for k, dest in enumerate(peers):
        ps_copy(k, dest).wait_send()

    @pl.loop(1, nz)
    def _(d):
        pq_copy(zmod(z + d), z).wait_send()

    finish(y, branch, post)
    for k, source in enumerate((y_far, y_left, y_right)):
        mo_copy(k, source).wait_recv()
        po_copy(k, source).wait_recv()
        finish(source, bfull[k].astype(F32), post_all[k])

    for k, dest in enumerate(peers):
        mo_copy(k, dest).wait_send()
        po_copy(k, dest).wait_send()


def local(tokens, pre_gain, w_gate, w_up, conv_gate, conv_up, w_down, post_gain):
    nz = lax.axis_size("ra")
    _, positions, kb = tokens.shape
    ff = w_gate.shape[1]
    units = ff // nz
    lanes = -(-2 * units // 128) * 128
    rows = kb // 8
    quarter = positions // 4
    subs = -(-units // (-(-units // 64) * 16))
    dim_full = kb * nz

    dma = pltpu.SemaphoreType.DMA
    vmem = pltpu.VMEM
    scratch = [
        vmem((positions, kb), BF16),
        vmem((1, kb), F32),
        vmem((1, kb), F32),
        vmem((positions, kb), BF16),
        vmem((1, positions), F32),
        vmem((nz, rows, lanes), BF16),
        vmem((2, rows, ff), BF16),
        vmem((ff, kb), BF16),
        vmem((3, ff), F32),
        vmem((3, ff), F32),
        vmem((8, ff), F32),
        vmem((ff, 8), F32),
        vmem((nz, positions, kb), BF16),
        vmem((nz, 8, rows, lanes), BF16),
        vmem((nz, units, positions), BF16),
        vmem((positions, lanes), F32),
        vmem((lanes, positions), F32),
        vmem((kb, positions), F32),
        vmem((3, kb, quarter), BF16),
        vmem((3, kb, quarter), BF16),
        vmem((nz, 1, positions), F32),
        vmem((1, quarter), F32),
        vmem((nz, 1, quarter), F32),
        vmem((quarter, kb), BF16),
        vmem((3, quarter, kb), BF16),
        vmem((1, quarter), F32),
        vmem((3, 1, quarter), F32),
        dma((8,)),
        dma((2, nz, 2)), dma((nz, 2)),
        dma((2, nz)), dma((2, nz)), dma((2, nz)), dma((2, nz)),
        dma((nz,)), dma((nz,)), dma((2, nz)), dma((2, nz)), dma((nz,)), dma((nz,)),
        dma((4, nz)), dma((4, nz)),
        dma((nz,)), dma((nz,)), dma((2, nz, subs)), dma((nz, subs)),
        dma((3,)), dma((3,)), dma((nz,)), dma((nz,)), dma((3,)), dma((3,)), dma((3,)), dma((3,)),
        pltpu.SemaphoreType.REGULAR, pltpu.SemaphoreType.REGULAR,
    ]

    here = pl.BlockSpec(memory_space=pltpu.VMEM)
    away = pl.BlockSpec(memory_space=pl.ANY)
    out = pl.pallas_call(
        functools.partial(_kernel, dim_full, nz),
        out_shape=jax.ShapeDtypeStruct((positions, kb), BF16),
        in_specs=[away] * 8,
        out_specs=pl.BlockSpec(memory_space=pltpu.VMEM),
        scratch_shapes=scratch,
        name="ffn",
        compiler_params=pltpu.CompilerParams(
            collective_id=0, has_side_effects=True, vmem_limit_bytes=67043328
        ),
    )(tokens[0], pre_gain[None, :], w_gate, w_up, conv_gate, conv_up, w_down, post_gain[None, :])
    return out[None]


def solution(mesh):
    in_specs = (
        P("dp", None, "ra"),
        P("ra"),
        P("ra", "cb"),
        P("ra", "cb"),
        P(None, "cb"),
        P(None, "cb"),
        P("cb", "ra"),
        P("ra"),
    )
    out_specs = P("dp", None, "ra")
    return jax.shard_map(local, mesh=mesh, in_specs=in_specs, out_specs=out_specs, check_vma=False)
```
